256 devices in a mesh: fs: 64 (over z, y, core), tp: 4 (over x).
Axes of the slice: x: 4, y: 4, z: 8, core: 2. Of those that a mesh axis runs over, the one named last changes fastest.
Arguments:
- tokens: bfloat16 [3072, 2048], P('tp'), may hold values from -6 to 6
- norm_gain: float32 [2048], P('fs'), may hold values from 0.1 to 1.9
- gate_weight: float32 [4, 2048, 8192], P(None, 'fs', 'tp'), may hold values from -0.125 to 0.125
- up_weight: float32 [4, 2048, 8192], P(None, 'fs', 'tp'), may hold values from -0.125 to 0.125
- down_weight: float32 [4, 8192, 2048], P(None, 'fs', 'tp'), may hold values from -0.0625 to 0.0625
- routes: int32 [3072, 2], P('tp'), may hold values from 0 to 3, all different within a row; in each aligned block of 768 rows (0 to 767, 768 to 1535, ...) at most 480 rows name the same one
- route_logit: float32 [3072, 2], P('tp'), may hold values from -6 to 6
Outputs:
- gate_out: bfloat16 [4, 2048, 8192], P(None, None, 'fs')
- up_out: bfloat16 [4, 2048, 8192], P(None, None, 'fs')
- down_out: bfloat16 [4, 8192, 2048], P(None, 'fs')
- mixed: bfloat16 [3072, 2048], P(('tp', 'fs'))
The draws below stay inside these ranges and needn't reach their ends.
Inputs may be any that keep to these rules, and one draw needn't show every extreme that they name: `routes`: the two experts of a token differ. In each aligned block of 768 tokens (the tokens of one request group) every expert is named by at most 480 tokens, a bound that some block reaches.
All inputs are finite; a program needn't handle non-finite values.
Results may differ from the reference program's by a relative error of at most 0.0082.
Values may be sent and summed in bfloat16 or wider, within the bound.
A program may use at most 128 MiB of HBM per device.

```python
import math
import jax
import jax.numpy as jnp
import numpy as np
from jax import lax

D = 2048
FF = 8192
E = 4
TOK_GROUP = 768
CAP = 480
TOKENS = 3072


def levels(stream_key, dims, shards, least, largest):
    factor_of = 1.0
    for axis_at, parts in shards:
        steps = jax.random.uniform(jax.random.fold_in(jax.random.fold_in(stream_key, 6), axis_at), (parts,), jnp.float32, least / len(shards), largest / len(shards))
        factor_of = factor_of * jnp.repeat(jnp.exp(steps), dims[axis_at] // parts).reshape((-1,) + (1,) * (len(dims) - 1 - axis_at))
    return factor_of


def deal_out(rng, own, number, rows, number_of, top, limit, skew):
    sequence = jax.random.permutation(rng, number_of)
    packed, ordinary = load_shares(number_of, rows * top, limit, skew, True), load_shares(number_of, rows * top, limit, skew, False)
    places = jnp.arange(number_of)

    def named(tallies, rotation):
        used = int((tallies > 0).sum())
        fixed = max(1, used // 4)
        passed = fixed + (places - fixed + rotation * (used - fixed)) % max(1, number_of - fixed)
        return jnp.zeros((number_of,), jnp.int32).at[sequence[jnp.where(places < fixed, places, passed)]].set(jnp.asarray(tallies, jnp.int32))

    tallies = jnp.where(number % 4 == 0, named(packed, number // 4), named(ordinary, number - number // 4 - 1))
    mixed = jax.random.permutation(jax.random.fold_in(own, 3), number_of)
    source_of, receiver = mixed[0:number_of // 2 * 2:2], mixed[1:number_of // 2 * 2:2]
    margin = jnp.minimum(tallies[source_of] - 1, limit - tallies[receiver]) // 2
    margin = jnp.where((source_of == sequence[0]) | (receiver == sequence[0]) | (tallies[receiver] == 0), 0, jnp.maximum(margin, 0))
    passed = jax.random.randint(jax.random.fold_in(own, 4), (number_of // 2,), 0, 1 << 20) % (margin + 1)
    tallies = tallies.at[source_of].add(-passed).at[receiver].add(passed)
    items = jnp.searchsorted(jnp.cumsum(tallies), jnp.arange(rows * top), side="right").astype(jnp.int32)
    grid = items.reshape(top, rows).T
    grid = grid[jax.random.permutation(jax.random.fold_in(own, 1), rows)]
    rotation = jax.random.randint(jax.random.fold_in(own, 2), (rows, 1), 0, top)
    return jnp.take_along_axis(grid, (jnp.arange(top)[None, :] + rotation) % top, axis=1)


def load_shares(amount, total, bound, skew, full):
    loads = [(1 << 20) // math.isqrt(grade ** skew) + 1 for grade in range(1, amount + 1)]
    largest = bound if full else min(bound, max(-(-total // amount), total * loads[0] // sum(loads)))
    least = 1 if total - largest >= amount - 1 else 0
    counts, spare = [largest] + [least] * (amount - 1), total - largest - least * (amount - 1)
    while spare > 0:
        movable = [i for i in range(1, amount) if counts[i] < largest] or [i for i in range(1, amount) if counts[i] < bound]
        pool, left = sum([loads[i] for i in movable]), spare
        for i in movable:
            more = min(bound - counts[i], max(1, left * loads[i] // pool), spare)
            counts[i] = counts[i] + more
            spare = spare - more
    return np.array(counts)


def scatter_about(stream_key, shape, deviation, limit, pieces=(), held_as=jnp.bfloat16):
    entries = jax.random.normal(stream_key, shape, jnp.float32) * deviation
    if len(pieces) > 0:
        entries = levels(stream_key, shape, pieces, -0.22, 0.18) * entries
    return jnp.clip(entries, min=-limit, max=limit).astype(held_as)


def setup_inputs(seed: int = 0) -> dict:
    seeds = jax.random.split(jax.random.key(seed), 8)
    tokens = scatter_about(seeds[0], (TOKENS, D), 1.0, 6.0, ((0, 4),))
    norm_gain = jnp.clip(1.0 + 0.18 * jax.random.normal(seeds[1], (D,), jnp.float32), 0.1, 1.9)
    gate_weight = scatter_about(seeds[2], (E, D, FF), D ** -0.5, 0.125, ((1, 64), (2, 4)), jnp.float32)
    up_weight = scatter_about(seeds[3], (E, D, FF), D ** -0.5, 0.125, ((1, 64), (2, 4)), jnp.float32)
    down_weight = scatter_about(seeds[4], (E, FF, D), FF ** -0.5, 0.0625, ((1, 64), (2, 4)), jnp.float32)
    routes_keys = jax.random.split(jax.random.fold_in(seeds[5], 1), TOKENS // TOK_GROUP)
    routes_turns = jax.random.permutation(jax.random.fold_in(seeds[5], 3), TOKENS // TOK_GROUP)
    routes = jax.vmap(lambda own, number: deal_out(jax.random.fold_in(seeds[5], 2), own, number, TOK_GROUP, E, 2, CAP, 1))(routes_keys, routes_turns).reshape((TOKENS, 2))
    route_logit = scatter_about(seeds[6], (TOKENS, 2), 1.0, 6.0, ((0, 4),), jnp.float32)
    return dict(tokens=tokens, norm_gain=norm_gain, gate_weight=gate_weight, up_weight=up_weight, down_weight=down_weight, routes=routes, route_logit=route_logit)


EPS = 0.5

def reference(tokens, norm_gain, gate_weight, up_weight, down_weight, routes, route_logit):
    gain_col = norm_gain.astype(jnp.float32)[None, :, None]
    gate_out = (gate_weight * gain_col).astype(jnp.bfloat16)
    up_out = (up_weight * gain_col).astype(jnp.bfloat16)
    down_out = down_weight.astype(jnp.bfloat16)
    floats = tokens.astype(jnp.float32)
    normed = (floats * lax.rsqrt(lax.optimization_barrier(jnp.mean(floats * floats, axis=1, keepdims=True)) + EPS)).astype(jnp.bfloat16)
    first_share = jax.nn.sigmoid(route_logit[:, 0] - route_logit[:, 1])
    shares = jnp.stack([first_share, 1.0 - first_share], axis=1)
    summed = jnp.zeros(tokens.shape, jnp.float32)
    for expert in range(E):
        weight_col = lax.optimization_barrier(jnp.sum(jnp.where(routes == expert, shares, 0.0), axis=1, keepdims=True))
        gate_val = jnp.dot(normed, gate_out[expert], preferred_element_type=jnp.float32)
        up_val = jnp.dot(normed, up_out[expert], preferred_element_type=jnp.float32)
        hidden = (jax.nn.silu(gate_val) * up_val).astype(jnp.bfloat16)
        result = jnp.dot(hidden, down_out[expert], preferred_element_type=jnp.float32)
        summed = summed + weight_col * result
    return (gate_out, up_out, down_out, summed.astype(jnp.bfloat16))
```

```python
import functools

import jax
import jax.numpy as jnp
from jax import lax
from jax.experimental import pallas as pl
from jax.experimental.pallas import tpu as pltpu
from jax.sharding import Mesh
from jax.sharding import PartitionSpec as P

FS = ("fs_0", "fs_1", "fs_2")
TP_FS = ("tp", "fs_0", "fs_1", "fs_2")
EPS = 0.5
MESH = pl.DeviceIdType.MESH


def weights_kernel(
    sizes,
    gate_ref,
    up_ref,
    gain_ref,
    down_ref,
    gate_out,
    up_out,
    down_out,
    staged,
    spread,
    by_z,
    a_send,
    a_recv,
    z_send,
    z_recv,
    y_send,
    y_recv,
    c_send,
    c_recv,
    f_send,
    f_recv,
):
    nz, ny, nc, nx = sizes
    nyc = ny * nc
    nk = nz * nyc
    per_x = nk // nx
    my_z, my_y = lax.axis_index("fs_0"), lax.axis_index("fs_1")
    my_c, my_x = lax.axis_index("fs_2"), lax.axis_index("tp")
    my_yc = my_y * nc + my_c
    outs = (gate_out, up_out)

    def at(dz=0, dy=0, dc=0, dx=0):
        return (
            lax.rem(my_z + dz, nz),
            lax.rem(my_y + dy, ny),
            lax.rem(my_c + dc, nc),
            lax.rem(my_x + dx, nx),
        )

    yc_steps = [(dy, dc) for dy in range(ny) for dc in range(nc) if dy + dc > 0]
    peers = (
        [at(dx=d) for d in range(1, nx)]
        + [at(dz=d) for d in range(1, nz)]
        + [at(dy=dy, dc=dc) for dy, dc in yc_steps]
    )
    barrier = pltpu.get_barrier_semaphore()
    for peer in peers:
        pl.semaphore_signal(barrier, inc=1, device_id=peer, device_id_type=MESH)

    def remote(src, dst, ssem, rsem, peer):
        return pltpu.make_async_remote_copy(
            src_ref=src, dst_ref=dst, send_sem=ssem, recv_sem=rsem, device_id=peer, device_id_type=MESH
        )

    rows = gate_ref.shape[1]
    width = gate_ref.shape[2] // per_x
    gain = gain_ref[...]

    def convert(m, ref):
        for d in range(nx):
            expert = lax.rem(my_x + d, nx)
            for k in range(per_x):
                block = (ref[expert, :, k * width : (k + 1) * width] * gain).astype(jnp.bfloat16)
                if d == 0:
                    spread[m, my_x * per_x + k] = block
                else:
                    staged[m, d, k] = block

    sent = []

    def start(copy):
        copy.start()
        sent.append(copy)
        return copy

    a_copies = {}
    for m, ref in ((0, gate_ref), (1, up_ref)):
        convert(m, ref)
        if m == 0:
            pl.semaphore_wait(barrier, len(peers))
        for d in range(1, nx):
            a_copies[m, d] = start(
                remote(
                    staged.at[m, d],
                    spread.at[m, pl.ds(my_x * per_x, per_x)],
                    a_send.at[m, d],
                    a_recv.at[m, d],
                    at(dx=d),
                )
            )
    cols = down_ref.shape[2]
    half_e = nx // 2
    own = pl.ds(pl.multiple_of(my_x * cols, cols), cols)
    for e in range(nx):
        down_out[e, :, own] = down_ref[e].astype(jnp.bfloat16)

    def ring(tag, block):
        near = {}
        for h in (0, 1):
            near[0, h] = start(
                remote(
                    block(my_x, h), block(my_x, h), c_send.at[tag, 0, h], c_recv.at[tag, 0, h], at(dx=1)
                )
            )
            g = 1 - h
            near[1, g] = start(
                remote(
                    block(my_x, g), block(my_x, g), c_send.at[tag, 1, g], c_recv.at[tag, 1, g], at(dx=nx - 1)
                )
            )
        return near

    def pass_on(tag, block, near):
        left, right = lax.rem(my_x + nx - 1, nx), lax.rem(my_x + 1, nx)
        near[0, 0].wait_recv()
        first = start(
            remote(block(left, 0), block(left, 0), f_send.at[tag, 0], f_recv.at[tag, 0], at(dx=1))
        )
        near[1, 1].wait_recv()
        second = start(
            remote(block(right, 1), block(right, 1), f_send.at[tag, 1], f_recv.at[tag, 1], at(dx=nx - 1))
        )
        return near[0, 1], near[1, 0], first, second

    def down_block(x, h):
        return down_out.at[
            pl.ds(h * half_e, half_e), :, pl.ds(pl.multiple_of(x * cols, cols), cols)
        ]

    down_near = ring(2, down_block)

    z_copies = {}
    for m in (0, 1):
        for d in range(1, nx):
            a_copies[m, d].wait_recv()
        for dz in range(1, nz):
            peer = at(dz=dz)
            z_copies[m, dz] = start(
                remote(
                    spread.at[m, pl.ds(peer[0] * nyc, nyc)],
                    by_z.at[m, my_z],
                    z_send.at[m, dz],
                    z_recv.at[m, dz],
                    peer,
                )
            )
        by_z[m, my_z] = spread[m, pl.ds(my_z * nyc, nyc)]

    y_copies = {}

    def exchange_yc(m):
        out = outs[m]
        for dz in range(1, nz):
            z_copies[m, dz].wait_recv()
        for i, (dy, dc) in enumerate(yc_steps):
            peer = at(dy=dy, dc=dc)
            y_copies[m, i] = start(
                remote(
                    by_z.at[m, :, peer[1] * nc + peer[2]],
                    out.at[my_x, :, my_yc],
                    y_send.at[m, i],
                    y_recv.at[m, i],
                    peer,
                )
            )
        out[my_x, :, my_yc] = by_z[m, :, my_yc]

    half_z = nz // 2

    def out_block(m):
        return lambda x, h: outs[m].at[x, pl.ds(h * half_z, half_z)]

    exchange_yc(0)
    down_rest = pass_on(2, down_block, down_near)
    for i in range(len(yc_steps)):
        y_copies[0, i].wait_recv()
    near0 = ring(0, out_block(0))
    exchange_yc(1)
    rest0 = pass_on(0, out_block(0), near0)
    for i in range(len(yc_steps)):
        y_copies[1, i].wait_recv()
    near1 = ring(1, out_block(1))
    rest1 = pass_on(1, out_block(1), near1)
    for copy in down_rest + rest0 + rest1:
        copy.wait_recv()
    for copy in sent:
        copy.wait_send()


def hand_over(sizes, gate_weight, up_weight, gain, down_weight):
    nz, ny, nc, nx = sizes
    nyc = ny * nc
    nk = nz * nyc
    per_x = nk // nx
    experts, rows, cols = gate_weight.shape
    width = cols // per_x
    hid, dcols = down_weight.shape[1:]
    bf = jnp.bfloat16
    steps = nyc - 1
    dma = pltpu.SemaphoreType.DMA
    vmem = pl.BlockSpec(memory_space=pltpu.VMEM)
    gate, up, down = pl.pallas_call(
        functools.partial(weights_kernel, sizes),
        out_shape=[
            jax.ShapeDtypeStruct((experts, nz, nyc, rows, width), bf),
            jax.ShapeDtypeStruct((experts, nz, nyc, rows, width), bf),
            jax.ShapeDtypeStruct((experts, hid, dcols * nx), bf),
        ],
        in_specs=[vmem] * 4,
        out_specs=[vmem] * 3,
        scratch_shapes=[
            pltpu.VMEM((2, nx, per_x, rows, width), bf),
            pltpu.VMEM((2, nk, rows, width), bf),
            pltpu.VMEM((2, nz, nyc, rows, width), bf),
            dma((2, nx)),
            dma((2, nx)),
            dma((2, nz)),
            dma((2, nz)),
            dma((2, steps)),
            dma((2, steps)),
            dma((3, 2, 2)),
            dma((3, 2, 2)),
            dma((3, 2)),
            dma((3, 2)),
        ],
        compiler_params=pltpu.CompilerParams(
            collective_id=0, has_side_effects=True, vmem_limit_bytes=60 * 1024 * 1024
        ),
        name="hand_over",
    )(gate_weight, up_weight, gain, down_weight)
    full = (experts, nk * rows, width)
    return gate.reshape(full), up.reshape(full), down


def sum_by_axis(so_far, axes):
    for axis in axes:
        so_far = lax.psum_scatter(so_far, axis, scatter_dimension=0, tiled=True)
    return so_far


def shards(sizes, tokens, norm_gain, gate_weight, up_weight, down_weight, routes, route_logit):
    gate_out, up_out, down_out = hand_over(
        sizes, gate_weight, up_weight, norm_gain[:, None], down_weight
    )
    experts = gate_out.shape[0]
    floats = tokens.astype(jnp.float32)
    normed = (floats * lax.rsqrt(jnp.mean(floats * floats, axis=1, keepdims=True) + EPS)).astype(
        jnp.bfloat16
    )
    first_share = jax.nn.sigmoid(route_logit[:, 0] - route_logit[:, 1])
    shares = jnp.stack([first_share, 1.0 - first_share], axis=1)
    parts = []
    for e in range(experts):
        weight = jnp.sum(jnp.where(routes == e, shares, 0.0), axis=1, keepdims=True)
        gate_val = jnp.dot(normed, gate_out[e], preferred_element_type=jnp.float32)
        up_val = jnp.dot(normed, up_out[e], preferred_element_type=jnp.float32)
        parts.append((jax.nn.silu(gate_val) * up_val * weight).astype(jnp.bfloat16))
    hidden = jnp.concatenate(parts, axis=1)
    partial = jnp.dot(
        hidden, down_out.reshape(-1, down_out.shape[2]), preferred_element_type=jnp.float32
    )
    mixed = sum_by_axis(partial, FS)
    return (gate_out, up_out, down_out, mixed.astype(jnp.bfloat16))


def solution(mesh):
    sizes = (8, 4, 2, mesh.shape["tp"])
    finer = Mesh(mesh.devices.reshape(sizes), ("fs_0", "fs_1", "fs_2", "tp"))
    in_specs = (
        P("tp", None),
        P(FS),
        P(None, FS, "tp"),
        P(None, FS, "tp"),
        P(None, FS, "tp"),
        P("tp", None),
        P("tp", None),
    )
    out_specs = (P(None, None, FS), P(None, None, FS), P(None, FS, None), P(TP_FS, None))
    return jax.shard_map(
        functools.partial(shards, sizes),
        mesh=finer,
        in_specs=in_specs,
        out_specs=out_specs,
        check_vma=False,
    )
```

```python
import functools

import jax
import jax.numpy as jnp
from jax import lax
from jax.experimental import pallas as pl
from jax.experimental.pallas import tpu as pltpu
from jax.sharding import Mesh
from jax.sharding import PartitionSpec as P

FS = ("fs_0", "fs_1", "fs_2")
TP_FS = ("tp", "fs_0", "fs_1", "fs_2")
EPS = 0.5
MESH = pl.DeviceIdType.MESH
MIB = 1024 * 1024
VMEM_ONE, VMEM_TWO, VMEM_THREE = 32 * MIB, 40 * MIB, 32 * MIB


def weights_kernel(
    sizes,
    gate_ref,
    up_ref,
    gain_ref,
    down_ref,
    token_ref,
    route_ref,
    logit_ref,
    gate_out,
    up_out,
    down_out,
    normed_out,
    share_out,
    staged,
    spread,
    by_z,
    a_send,
    a_recv,
    z_send,
    z_recv,
    y_send,
    y_recv,
    c_send,
    c_recv,
    f_send,
    f_recv,
):
    nz, ny, nc, nx = sizes
    nyc = ny * nc
    nk = nz * nyc
    per_x = nk // nx
    my_z, my_y = lax.axis_index("fs_0"), lax.axis_index("fs_1")
    my_c, my_x = lax.axis_index("fs_2"), lax.axis_index("tp")
    my_yc = my_y * nc + my_c
    outs = (gate_out, up_out)

    def at(dz=0, dy=0, dc=0, dx=0):
        return (
            lax.rem(my_z + dz, nz),
            lax.rem(my_y + dy, ny),
            lax.rem(my_c + dc, nc),
            lax.rem(my_x + dx, nx),
        )

    yc_steps = [(dy, dc) for dy in range(ny) for dc in range(nc) if dy + dc > 0]
    peers = (
        [at(dx=d) for d in range(1, nx)]
        + [at(dz=d) for d in range(1, nz)]
        + [at(dy=dy, dc=dc) for dy, dc in yc_steps]
    )
    barrier = pltpu.get_barrier_semaphore()
    for peer in peers:
        pl.semaphore_signal(barrier, inc=1, device_id=peer, device_id_type=MESH)

    def remote(src, dst, ssem, rsem, peer):
        return pltpu.make_async_remote_copy(
            src_ref=src, dst_ref=dst, send_sem=ssem, recv_sem=rsem, device_id=peer, device_id_type=MESH
        )

    rows = gate_ref.shape[1]
    width = gate_ref.shape[2] // per_x
    gain = gain_ref[...]

    def convert(m, ref):
        for d in range(nx):
            expert = lax.rem(my_x + d, nx)
            for k in range(per_x):
                block = (ref[expert, :, k * width : (k + 1) * width] * gain).astype(jnp.bfloat16)
                if d == 0:
                    spread[m, my_x * per_x + k] = block
                else:
                    staged[m, d, k] = block

    sent = []

    def start(copy):
        copy.start()
        sent.append(copy)
        return copy

    a_copies = {}
    for m, ref in ((0, gate_ref), (1, up_ref)):
        convert(m, ref)
        if m == 0:
            pl.semaphore_wait(barrier, len(peers))
        for d in range(1, nx):
            a_copies[m, d] = start(
                remote(
                    staged.at[m, d],
                    spread.at[m, pl.ds(my_x * per_x, per_x)],
                    a_send.at[m, d],
                    a_recv.at[m, d],
                    at(dx=d),
                )
            )
    cols = down_ref.shape[2]
    half_e = nx // 2
    own = pl.ds(pl.multiple_of(my_x * cols, cols), cols)
    for e in range(nx):
        down_out[e, :, own] = down_ref[e].astype(jnp.bfloat16)

    def ring(tag, block):
        near = {}
        for h in (0, 1):
            near[0, h] = start(
                remote(
                    block(my_x, h), block(my_x, h), c_send.at[tag, 0, h], c_recv.at[tag, 0, h], at(dx=1)
                )
            )
            g = 1 - h
            near[1, g] = start(
                remote(
                    block(my_x, g), block(my_x, g), c_send.at[tag, 1, g], c_recv.at[tag, 1, g], at(dx=nx - 1)
                )
            )
        return near

    def pass_on(tag, block, near):
        left, right = lax.rem(my_x + nx - 1, nx), lax.rem(my_x + 1, nx)
        near[0, 0].wait_recv()
        first = start(
            remote(block(left, 0), block(left, 0), f_send.at[tag, 0], f_recv.at[tag, 0], at(dx=1))
        )
        near[1, 1].wait_recv()
        second = start(
            remote(block(right, 1), block(right, 1), f_send.at[tag, 1], f_recv.at[tag, 1], at(dx=nx - 1))
        )
        return near[0, 1], near[1, 0], first, second

    def down_block(x, h):
        return down_out.at[
            pl.ds(h * half_e, half_e), :, pl.ds(pl.multiple_of(x * cols, cols), cols)
        ]

    down_near = ring(2, down_block)

    step = 48
    def norm_rows(i, carry):
        at_rows = pl.ds(pl.multiple_of(i * step, step), step)
        floats = token_ref[at_rows, :].astype(jnp.float32)
        scale = lax.rsqrt(jnp.mean(floats * floats, axis=1, keepdims=True) + EPS)
        normed_out[at_rows, :] = (floats * scale).astype(jnp.bfloat16)
        return carry

    lax.fori_loop(0, token_ref.shape[0] // step, norm_rows, 0)
    first = 1.0 / (1.0 + jnp.exp(logit_ref[1:2, :] - logit_ref[0:1, :]))
    lines = [
        jnp.where(route_ref[0:1, :] == e, first, 0.0)
        + jnp.where(route_ref[1:2, :] == e, 1.0 - first, 0.0)
        for e in range(nx)
    ]
    lines.append(jnp.zeros((128 - nx, first.shape[1]), jnp.float32))
    share_out[...] = jnp.concatenate(lines, axis=0).T

    z_copies = {}
    for m in (0, 1):
        for d in range(1, nx):
            a_copies[m, d].wait_recv()
        for dz in range(1, nz):
            peer = at(dz=dz)
            z_copies[m, dz] = start(
                remote(
                    spread.at[m, pl.ds(peer[0] * nyc, nyc)],
                    by_z.at[m, my_z],
                    z_send.at[m, dz],
                    z_recv.at[m, dz],
                    peer,
                )
            )
        by_z[m, my_z] = spread[m, pl.ds(my_z * nyc, nyc)]

    y_copies = {}

    def exchange_yc(m):
        out = outs[m]
        for dz in range(1, nz):
            z_copies[m, dz].wait_recv()
        for i, (dy, dc) in enumerate(yc_steps):
            peer = at(dy=dy, dc=dc)
            y_copies[m, i] = start(
                remote(
                    by_z.at[m, :, peer[1] * nc + peer[2]],
                    out.at[my_x, :, my_yc],
                    y_send.at[m, i],
                    y_recv.at[m, i],
                    peer,
                )
            )
        out[my_x, :, my_yc] = by_z[m, :, my_yc]

    half_z = nz // 2

    def out_block(m):
        return lambda x, h: outs[m].at[x, pl.ds(h * half_z, half_z)]

    exchange_yc(0)
    down_rest = pass_on(2, down_block, down_near)
    for i in range(len(yc_steps)):
        y_copies[0, i].wait_recv()
    near0 = ring(0, out_block(0))
    exchange_yc(1)
    rest0 = pass_on(0, out_block(0), near0)
    for i in range(len(yc_steps)):
        y_copies[1, i].wait_recv()
    near1 = ring(1, out_block(1))
    rest1 = pass_on(1, out_block(1), near1)
    for copy in down_rest + rest0 + rest1:
        copy.wait_recv()
    for copy in sent:
        copy.wait_send()


def hand_over(sizes, gate_weight, up_weight, gain, down_weight, tokens, routes, logits):
    nz, ny, nc, nx = sizes
    nyc = ny * nc
    nk = nz * nyc
    per_x = nk // nx
    experts, rows, cols = gate_weight.shape
    width = cols // per_x
    hid, dcols = down_weight.shape[1:]
    bf = jnp.bfloat16
    steps = nyc - 1
    dma = pltpu.SemaphoreType.DMA
    vmem = pl.BlockSpec(memory_space=pltpu.VMEM)
    gate, up, down, normed, share = pl.pallas_call(
        functools.partial(weights_kernel, sizes),
        out_shape=[
            jax.ShapeDtypeStruct((experts, nz, nyc, rows, width), bf),
            jax.ShapeDtypeStruct((experts, nz, nyc, rows, width), bf),
            jax.ShapeDtypeStruct((experts, hid, dcols * nx), bf),
            jax.ShapeDtypeStruct(tokens.shape, bf),
            jax.ShapeDtypeStruct((tokens.shape[0], 128), jnp.float32),
        ],
        in_specs=[vmem] * 7,
        out_specs=[vmem] * 5,
        scratch_shapes=[
            pltpu.VMEM((2, nx, per_x, rows, width), bf),
            pltpu.VMEM((2, nk, rows, width), bf),
            pltpu.VMEM((2, nz, nyc, rows, width), bf),
            dma((2, nx)),
            dma((2, nx)),
            dma((2, nz)),
            dma((2, nz)),
            dma((2, steps)),
            dma((2, steps)),
            dma((3, 2, 2)),
            dma((3, 2, 2)),
            dma((3, 2)),
            dma((3, 2)),
        ],
        compiler_params=pltpu.CompilerParams(
            collective_id=0, has_side_effects=True, vmem_limit_bytes=VMEM_ONE
        ),
        name="hand_over",
    )(gate_weight, up_weight, gain, down_weight, tokens, routes, logits)
    full = (experts, nk * rows, width)
    return gate.reshape(full), up.reshape(full), down, normed, share


def compute_kernel(
    sizes, wy, gate_ref, up_ref, down_ref, x_ref, share_ref, gate_out, up_out, down_out, pz, py, sems
):
    nz, ny, nc, nx = sizes
    pairs = ((gate_ref, gate_out), (up_ref, up_out), (down_ref, down_out))
    copies = [pltpu.make_async_copy(a, b, sems.at[i]) for i, (a, b) in enumerate(pairs)]
    for copy in copies:
        copy.start()
    experts, hid, width = down_ref.shape
    half = width // nc
    tiles = 2 if nz % 2 == 0 else 1
    z_per = nz // tiles
    rows = x_ref.shape[0] // tiles
    r = x_ref.shape[0] // (nz * ny)

    def tile(t, carry):
        at_rows = pl.ds(pl.multiple_of(t * rows, rows), rows)
        x = x_ref[at_rows, :]
        parts = []
        for e in range(experts):
            both = jnp.concatenate([gate_ref[e], up_ref[e]], axis=1)
            val = jnp.dot(x, both, preferred_element_type=jnp.float32)
            gate_val, up_val = val[:, :hid], val[:, hid:]
            weight = share_ref[at_rows, e : e + 1]
            hidden = gate_val / (1.0 + jnp.exp(-gate_val)) * up_val
            parts.append(jnp.where(weight > 0.0, hidden * weight, 0.0).astype(jnp.bfloat16))
        hidden = jnp.concatenate(parts, axis=1)
        down = down_ref[...].reshape(experts * hid, width)
        for c in range(nc):
            lo = c * half
            val = jnp.dot(hidden, down[:, lo : lo + wy], preferred_element_type=jnp.float32)
            val = val.reshape(z_per, ny, r, wy).astype(jnp.bfloat16)
            for y in range(ny):
                py[c, y, pl.ds(t * z_per, z_per)] = val[:, y]
            val = jnp.dot(hidden, down[:, lo + wy : lo + half], preferred_element_type=jnp.float32)
            pz[c, pl.ds(t * z_per, z_per)] = val.reshape(z_per, ny, r, half - wy).astype(jnp.bfloat16)
        return carry

    lax.fori_loop(0, tiles, tile, 0)
    for copy in copies:
        copy.wait()


def compute(sizes, wy, gate, up, down, normed, share):
    nz, ny, nc, nx = sizes
    bf = jnp.bfloat16
    vmem = pl.BlockSpec(memory_space=pltpu.VMEM)
    hbm = pl.BlockSpec(memory_space=pl.ANY)
    r = normed.shape[0] // (nz * ny)
    half = down.shape[2] // nc
    return pl.pallas_call(
        functools.partial(compute_kernel, sizes, wy),
        out_shape=[
            jax.ShapeDtypeStruct(gate.shape, bf),
            jax.ShapeDtypeStruct(up.shape, bf),
            jax.ShapeDtypeStruct(down.shape, bf),
            jax.ShapeDtypeStruct((nc, nz, ny, r, half - wy), bf),
            jax.ShapeDtypeStruct((nc, ny, nz, r, wy), bf),
        ],
        in_specs=[vmem] * 5,
        out_specs=[hbm] * 3 + [vmem] * 2,
        scratch_shapes=[pltpu.SemaphoreType.DMA((3,))],
        compiler_params=pltpu.CompilerParams(vmem_limit_bytes=VMEM_TWO),
        name="experts",
    )(gate, up, down, normed, share)


def reduce_kernel(
    sizes,
    pz,
    py,
    out,
    cz,
    cy,
    sz,
    sy,
    rz,
    ry,
    tz,
    ty,
    qz,
    qy,
    whole,
    other,
    last,
    c_send,
    c_recv,
    z_send,
    z_recv,
    y_send,
    y_recv,
):
    nz, ny, nc, nx = sizes
    my_z, my_y = lax.axis_index("fs_0"), lax.axis_index("fs_1")
    my_c, my_x = lax.axis_index("fs_2"), lax.axis_index("tp")
    f32, bf = jnp.float32, jnp.bfloat16

    def at(dz=0, dy=0, dc=0):
        return (
            lax.rem(my_z + dz, nz),
            lax.rem(my_y + dy, ny),
            lax.rem(my_c + dc, nc),
            my_x,
        )

    twin = at(dc=1)
    z_peers = [at(dz=d) for d in range(nz)]
    y_peers = [at(dy=d) for d in range(ny)]
    peers = [twin] + z_peers[1:] + y_peers[1:]
    barrier = pltpu.get_barrier_semaphore()
    for peer in peers:
        pl.semaphore_signal(barrier, inc=1, device_id=peer, device_id_type=MESH)
    pl.semaphore_wait(barrier, len(peers))

    sent = []

    def start(src, dst, ssem, rsem, peer):
        copy = pltpu.make_async_remote_copy(
            src_ref=src, dst_ref=dst, send_sem=ssem, recv_sem=rsem, device_id=peer, device_id_type=MESH
        )
        copy.start()
        sent.append(copy)
        return copy

    twin_c = twin[2]
    c_z = start(pz.at[twin_c], cz, c_send.at[0], c_recv.at[0], twin)
    c_y = start(py.at[twin_c], cy, c_send.at[1], c_recv.at[1], twin)
    c_z.wait_recv()
    z1 = []
    for d in range(1, nz):
        z = z_peers[d][0]
        sz[z] = (pz[my_c, z].astype(f32) + cz[z].astype(f32)).astype(bf)
        z1.append(start(sz.at[z], rz.at[d], z_send.at[0, d], z_recv.at[0, d], z_peers[d]))
    c_y.wait_recv()
    y1 = []
    for d in range(1, ny):
        y = y_peers[d][1]
        for z in range(nz):
            sy[y, z] = (py[my_c, y, z].astype(f32) + cy[y, z].astype(f32)).astype(bf)
        y1.append(start(sy.at[y], ry.at[d], y_send.at[0, d], y_recv.at[0, d], y_peers[d]))
    for copy in y1:
        copy.wait_recv()

    def sum_y(z):
        total = py[my_c, my_y, z].astype(f32) + cy[my_y, z].astype(f32)
        for d in range(1, ny):
            total = total + ry[d, z].astype(f32)
        return total

    y2 = []
    for d in range(1, nz):
        z = z_peers[d][0]
        ty[z] = sum_y(z).astype(bf)
        y2.append(start(ty.at[z], qy.at[d], z_send.at[1, d], z_recv.at[1, d], z_peers[d]))
    for copy in z1:
        copy.wait_recv()

    def sum_z(y):
        total = pz[my_c, my_z, y].astype(f32) + cz[my_z, y].astype(f32)
        for d in range(1, nz):
            total = total + rz[d, y].astype(f32)
        return total

    z2 = []
    for d in range(1, ny):
        y = y_peers[d][1]
        tz[y] = sum_z(y).astype(bf)
        z2.append(start(tz.at[y], qz.at[d], y_send.at[1, d], y_recv.at[1, d], y_peers[d]))
    sum_of_z = sum_z(my_y)
    sum_of_y = sum_y(my_z)
    for d, copy in zip(range(1, ny), z2):
        copy.wait_recv()
        sum_of_z = sum_of_z + qz[d].astype(f32)
    for d, copy in zip(range(1, nz), y2):
        copy.wait_recv()
        sum_of_y = sum_of_y + qy[d].astype(f32)
    whole[...] = jnp.concatenate([sum_of_y, sum_of_z], axis=1)
    own = out.shape[0]
    low, high = whole[0:own, :], whole[own : 2 * own, :]
    first_core = my_c == 0
    other[...] = jnp.where(first_core, high, low)
    swap = start(other, last, c_send.at[2], c_recv.at[2], twin)
    mine = jnp.where(first_core, low, high)
    swap.wait_recv()
    theirs = last[...]
    left = jnp.where(first_core, mine, theirs)
    right = jnp.where(first_core, theirs, mine)
    out[...] = jnp.concatenate([left, right], axis=1).astype(out.dtype)
    for copy in sent:
        copy.wait_send()


def reduce_scatter(sizes, pz, py):
    nz, ny, nc, nx = sizes
    r, wz = pz.shape[3:]
    wy = py.shape[4]
    own, half = r // nc, wy + wz
    bf, f32 = jnp.bfloat16, jnp.float32
    dma = pltpu.SemaphoreType.DMA
    vmem = pl.BlockSpec(memory_space=pltpu.VMEM)
    return pl.pallas_call(
        functools.partial(reduce_kernel, sizes),
        out_shape=jax.ShapeDtypeStruct((own, half * nc), bf),
        in_specs=[vmem] * 2,
        out_specs=vmem,
        scratch_shapes=[
            pltpu.VMEM((nz, ny, r, wz), bf),
            pltpu.VMEM((ny, nz, r, wy), bf),
            pltpu.VMEM((nz, ny, r, wz), bf),
            pltpu.VMEM((ny, nz, r, wy), bf),
            pltpu.VMEM((nz, ny, r, wz), bf),
            pltpu.VMEM((ny, nz, r, wy), bf),
            pltpu.VMEM((ny, r, wz), bf),
            pltpu.VMEM((nz, r, wy), bf),
            pltpu.VMEM((ny, r, wz), bf),
            pltpu.VMEM((nz, r, wy), bf),
            pltpu.VMEM((r, half), f32),
            pltpu.VMEM((own, half), f32),
            pltpu.VMEM((own, half), f32),
            dma((3,)),
            dma((3,)),
            dma((2, nz)),
            dma((2, nz)),
            dma((2, ny)),
            dma((2, ny)),
        ],
        compiler_params=pltpu.CompilerParams(
            collective_id=1, has_side_effects=True, vmem_limit_bytes=VMEM_THREE
        ),
        name="sum_up",
    )(pz, py)


def shards(sizes, tokens, norm_gain, gate_weight, up_weight, down_weight, routes, route_logit):
    gate, up, down, normed, share = hand_over(
        sizes, gate_weight, up_weight, norm_gain[:, None], down_weight, tokens, routes.T, route_logit.T
    )
    wy = tokens.shape[1] // sizes[2] * 5 // 8
    gate_out, up_out, down_out, pz, py = compute(sizes, wy, gate, up, down, normed, share)
    return (gate_out, up_out, down_out, reduce_scatter(sizes, pz, py))


def solution(mesh):
    sizes = (8, 4, 2, mesh.shape["tp"])
    finer = Mesh(mesh.devices.reshape(sizes), ("fs_0", "fs_1", "fs_2", "tp"))
    in_specs = (
        P("tp", None),
        P(FS),
        P(None, FS, "tp"),
        P(None, FS, "tp"),
        P(None, FS, "tp"),
        P("tp", None),
        P("tp", None),
    )
    out_specs = (P(None, None, FS), P(None, None, FS), P(None, FS, None), P(TP_FS, None))
    return jax.shard_map(
        functools.partial(shards, sizes),
        mesh=finer,
        in_specs=in_specs,
        out_specs=out_specs,
        check_vma=False,
    )
```

```python
import functools

import jax
import jax.numpy as jnp
from jax import lax
from jax.experimental import pallas as pl
from jax.experimental.pallas import tpu as pltpu
from jax.sharding import Mesh
from jax.sharding import PartitionSpec as P

FS = ("fs_0", "fs_1", "fs_2")
TP_FS = ("tp", "fs_0", "fs_1", "fs_2")
EPS = 0.5
MESH = pl.DeviceIdType.MESH
MIB = 1024 * 1024
PARTS = 2


def whole_kernel(
    sizes,
    gate_hbm,
    up_hbm,
    gain_ref,
    down_hbm,
    token_hbm,
    route_ref,
    logit_ref,
    gate_out,
    up_out,
    down_out,
    mixed_out,
    gate_in,
    up_in,
    down_in,
    token_in,
    staged,
    spread,
    by_z,
    normed,
    share,
    hidden,
    part,
    from_twin,
    to_y,
    from_y,
    to_z,
    from_z,
    total,
    other,
    last,
    in_sem,
    a_send,
    a_recv,
    z_send,
    z_recv,
    y_send,
    y_recv,
    c_send,
    c_recv,
    f_send,
    f_recv,
    t_send,
    t_recv,
    ry_send,
    ry_recv,
    rz_send,
    rz_recv,
):
    nz, ny, nc, nx = sizes
    nyc = ny * nc
    nk = nz * nyc
    per_x = nk // nx
    f32, bf = jnp.float32, jnp.bfloat16
    my_z, my_y = lax.axis_index("fs_0"), lax.axis_index("fs_1")
    my_c, my_x = lax.axis_index("fs_2"), lax.axis_index("tp")
    my_yc = my_y * nc + my_c
    outs = (gate_out, up_out)

    loads = [
        pltpu.make_async_copy(src, dst, in_sem.at[i])
        for i, (src, dst) in enumerate(
            ((gate_hbm, gate_in), (up_hbm, up_in), (down_hbm, down_in), (token_hbm, token_in))
        )
    ]
    for load in loads:
        load.start()

    def at(dz=0, dy=0, dc=0, dx=0):
        return (
            lax.rem(my_z + dz, nz),
            lax.rem(my_y + dy, ny),
            lax.rem(my_c + dc, nc),
            lax.rem(my_x + dx, nx),
        )

    yc_steps = [(dy, dc) for dy in range(ny) for dc in range(nc) if dy + dc > 0]
    peers = (
        [at(dx=d) for d in range(1, nx)]
        + [at(dz=d) for d in range(1, nz)]
        + [at(dy=dy, dc=dc) for dy, dc in yc_steps]
    )
    barrier = pltpu.get_barrier_semaphore()
    for peer in peers:
        pl.semaphore_signal(barrier, inc=1, device_id=peer, device_id_type=MESH)

    sent = []

    def start(src, dst, ssem, rsem, peer):
        copy = pltpu.make_async_remote_copy(
            src_ref=src, dst_ref=dst, send_sem=ssem, recv_sem=rsem, device_id=peer, device_id_type=MESH
        )
        copy.start()
        sent.append(copy)
        return copy

    rows = gate_in.shape[1]
    width = gate_in.shape[2] // per_x
    sub = rows // PARTS
    gain_row = gain_ref[...]
    same = lax.broadcasted_iota(jnp.int32, (rows, rows), 0) == lax.broadcasted_iota(
        jnp.int32, (rows, rows), 1
    )
    gain = jnp.sum(jnp.where(same, gain_row, 0.0), axis=1, keepdims=True)
    chunks = [(m, h) for m in (0, 1) for h in range(PARTS)]

    a_copies = {}
    for m, ref in ((0, gate_in), (1, up_in)):
        loads[m].wait()
        for h in range(PARTS):
            lo = h * sub
            for d in range(nx):
                expert = lax.rem(my_x + d, nx)
                for k in range(per_x):
                    block = ref[expert, lo : lo + sub, k * width : (k + 1) * width]
                    block = (block * gain[lo : lo + sub]).astype(bf)
                    if d == 0:
                        spread[m, h, my_x * per_x + k] = block
                    else:
                        staged[m, h, d, k] = block
            if m + h == 0:
                pl.semaphore_wait(barrier, len(peers))
            for d in range(1, nx):
                a_copies[m, h, d] = start(
                    staged.at[m, h, d],
                    spread.at[m, h, pl.ds(my_x * per_x, per_x)],
                    a_send.at[m, h, d],
                    a_recv.at[m, h, d],
                    at(dx=d),
                )

    cols = down_in.shape[2]
    half_e = nx // 2
    loads[2].wait()
    own_cols = pl.ds(pl.multiple_of(my_x * cols, cols), cols)
    for e in range(nx):
        down_out[e, :, own_cols] = down_in[e].astype(bf)

    left, right = lax.rem(my_x + nx - 1, nx), lax.rem(my_x + 1, nx)

    def near(tag, block, side, h):
        ref = block(my_x, h)
        return start(
            ref, ref, c_send.at[tag, side, h], c_recv.at[tag, side, h], at(dx=1 if side == 0 else nx - 1)
        )

    def pass_on(tag, block, side):
        ref = block(left if side == 0 else right, side)
        return start(
            ref, ref, f_send.at[tag, side], f_recv.at[tag, side], at(dx=1 if side == 0 else nx - 1)
        )

    def down_block(x, h):
        return down_out.at[
            pl.ds(h * half_e, half_e), :, pl.ds(pl.multiple_of(x * cols, cols), cols)
        ]

    d_tag = len(chunks)
    d_near = {(s, s): near(d_tag, down_block, s, s) for s in (0, 1)}

    loads[3].wait()
    step = 48

    def norm_rows(i, carry):
        at_rows = pl.ds(pl.multiple_of(i * step, step), step)
        floats = token_in[at_rows, :].astype(f32)
        scale = lax.rsqrt(jnp.mean(floats * floats, axis=1, keepdims=True) + EPS)
        normed[at_rows, :] = (floats * scale).astype(bf)
        return carry

    lax.fori_loop(0, token_in.shape[0] // step, norm_rows, 0)
    first = 1.0 / (1.0 + jnp.exp(logit_ref[1:2, :] - logit_ref[0:1, :]))
    lines = [
        jnp.where(route_ref[0:1, :] == e, first, 0.0)
        + jnp.where(route_ref[1:2, :] == e, 1.0 - first, 0.0)
        for e in range(nx)
    ]
    lines.append(jnp.zeros((128 - nx, first.shape[1]), f32))
    columns = jnp.concatenate(lines, axis=0).T
    for e in range(nx):
        share[e] = jnp.broadcast_to(columns[:, e : e + 1], share.shape[1:])

    z_copies, y_copies, c_near, c_far = {}, {}, {}, {}
    half_z = nz // 2

    def over_z(q):
        m, h = q
        for d in range(1, nx):
            a_copies[m, h, d].wait_recv()
        for dz in range(1, nz):
            peer = at(dz=dz)
            z_copies[q, dz] = start(
                spread.at[m, h, pl.ds(peer[0] * nyc, nyc)],
                by_z.at[m, h, my_z],
                z_send.at[m, h, dz],
                z_recv.at[m, h, dz],
                peer,
            )
        by_z[m, h, my_z] = spread[m, h, pl.ds(my_z * nyc, nyc)]

    def over_yc(q):
        m, h = q
        out, lo = outs[m], h * sub
        for dz in range(1, nz):
            z_copies[q, dz].wait_recv()
        for i, (dy, dc) in enumerate(yc_steps):
            peer = at(dy=dy, dc=dc)
            y_copies[q, i] = start(
                by_z.at[m, h, :, peer[1] * nc + peer[2]],
                out.at[my_x, :, my_yc, pl.ds(lo, sub)],
                y_send.at[m, h, i],
                y_recv.at[m, h, i],
                peer,
            )
        out[my_x, :, my_yc, lo : lo + sub, :] = by_z[m, h, :, my_yc]

    def out_block(q):
        m, h = q
        return lambda x, half: outs[m].at[x, pl.ds(half * half_z, half_z), :, pl.ds(h * sub, sub)]

    def over_x(q):
        tag = chunks.index(q)
        for i in range(len(yc_steps)):
            y_copies[q, i].wait_recv()
        for s in (0, 1):
            c_near[q, s, s] = near(tag, out_block(q), s, s)
        for s in (0, 1):
            c_near[q, s, 1 - s] = near(tag, out_block(q), s, 1 - s)

    def onward(q):
        for s in (0, 1):
            c_near[q, s, s].wait_recv()
            c_far[q, s] = pass_on(chunks.index(q), out_block(q), s)

    experts = nx
    hid = width
    tiles = 2
    tile_rows = normed.shape[0] // tiles
    z_per = nz // tiles
    r = normed.shape[0] // (nz * ny)

    def run_expert(e):
        def tile(t, carry):
            at_rows = pl.ds(pl.multiple_of(t * tile_rows, tile_rows), tile_rows)
            shape = (nk * rows, width)
            both = jnp.concatenate([gate_out[e].reshape(shape), up_out[e].reshape(shape)], axis=1)
            val = jnp.dot(normed[at_rows, :], both, preferred_element_type=f32)
            gate_val, up_val = val[:, :hid], val[:, hid:]
            weight = share[e, at_rows, :]
            value = gate_val / (1.0 + jnp.exp(-gate_val)) * up_val
            hidden[e, at_rows, :] = jnp.where(weight > 0.0, value * weight, 0.0).astype(bf)
            return carry

        lax.fori_loop(0, tiles, tile, 0)

    q0, q1, q2, q3 = chunks
    over_z(q0)
    over_z(q1)
    over_z(q2)
    over_yc(q0)
    over_z(q3)
    over_x(q0)
    over_yc(q1)
    onward(q0)
    over_x(q1)
    over_yc(q2)
    onward(q1)
    over_x(q2)
    over_yc(q3)
    onward(q2)
    over_x(q3)
    run_expert(my_x)
    onward(q3)
    for s in (0, 1):
        d_near[s, 1 - s] = near(d_tag, down_block, s, 1 - s)
    d_far = []
    for s in (0, 1):
        d_near[s, s].wait_recv()
        d_far.append(pass_on(d_tag, down_block, s))
    for s, e in ((0, left), (1, right)):
        for q in chunks:
            c_near[q, s, 1 - s].wait_recv()
        run_expert(e)
    for q in chunks:
        for s in (0, 1):
            c_far[q, s].wait_recv()
    run_expert(lax.rem(my_x + nx // 2, nx))

    half = cols // nc
    twin = at(dc=1)
    y_peers = [at(dy=d) for d in range(ny)]
    z_peers = [at(dz=d) for d in range(nz)]
    blocks = [my_x, left, right, lax.rem(my_x + nx // 2, nx)]
    twin_copies, sum_y_copies, sum_z_copies = {}, {}, {}

    def multiply(b):
        at_cols = pl.ds(pl.multiple_of(blocks[b] * cols, cols), cols)

        def tile(t, carry):
            at_rows = pl.ds(pl.multiple_of(t * tile_rows, tile_rows), tile_rows)
            units = jnp.concatenate([hidden[e, at_rows, :] for e in range(experts)], axis=1)
            down = down_out[:, :, at_cols].reshape(experts * hid, cols)
            val = jnp.dot(units, down, preferred_element_type=f32)
            val = val.reshape(z_per, ny, r, cols).astype(bf)
            for c in range(nc):
                for y in range(ny):
                    part[b, c, y, pl.ds(t * z_per, z_per)] = val[:, y, :, c * half : (c + 1) * half]
            return carry

        lax.fori_loop(0, tiles, tile, 0)
        twin_copies[b] = start(
            part.at[b, twin[2]], from_twin.at[b], t_send.at[b], t_recv.at[b], twin
        )

    def sum_over_y(b):
        twin_copies[b].wait_recv()
        for d in range(1, ny):
            y = y_peers[d][1]
            to_y[b, y] = (part[b, my_c, y].astype(f32) + from_twin[b, y].astype(f32)).astype(bf)
            sum_y_copies[b, d] = start(
                to_y.at[b, y], from_y.at[b, d], ry_send.at[b, d], ry_recv.at[b, d], y_peers[d]
            )

    def summed(b, z):
        value = part[b, my_c, my_y, z].astype(f32) + from_twin[b, my_y, z].astype(f32)
        for d in range(1, ny):
            value = value + from_y[b, d, z].astype(f32)
        return value

    def sum_over_z(b):
        for d in range(1, ny):
            sum_y_copies[b, d].wait_recv()
        for d in range(1, nz):
            z = z_peers[d][0]
            to_z[b, z] = summed(b, z).astype(bf)
            sum_z_copies[b, d] = start(
                to_z.at[b, z], from_z.at[b, d], rz_send.at[b, d], rz_recv.at[b, d], z_peers[d]
            )

    def finish(b):
        value = summed(b, my_z)
        for d in range(1, nz):
            sum_z_copies[b, d].wait_recv()
            value = value + from_z[b, d].astype(f32)
        total[b] = value

    multiply(0)
    d_near[0, 1].wait_recv()
    multiply(1)
    sum_over_y(0)
    d_near[1, 0].wait_recv()
    multiply(2)
    sum_over_y(1)
    sum_over_z(0)
    sum_over_y(2)
    for copy in d_far:
        copy.wait_recv()
    multiply(3)
    sum_over_z(1)
    sum_over_y(3)
    finish(0)
    sum_over_z(2)
    finish(1)
    sum_over_z(3)
    finish(2)
    finish(3)

    own = mixed_out.shape[0]
    first_core = my_c == 0
    low, high = total[:, 0:own, :], total[:, own : 2 * own, :]
    other[...] = jnp.where(first_core, high, low)
    swap = start(other, last, t_send.at[len(blocks)], t_recv.at[len(blocks)], twin)
    mine = jnp.where(first_core, low, high)
    swap.wait_recv()
    theirs = last[...]
    for b, x in enumerate(blocks):
        pair = [
            jnp.where(first_core, mine[b], theirs[b]),
            jnp.where(first_core, theirs[b], mine[b]),
        ]
        at_cols = pl.ds(pl.multiple_of(x * cols, cols), cols)
        mixed_out[:, at_cols] = jnp.concatenate(pair, axis=1).astype(bf)
    for copy in sent:
        copy.wait_send()


def away(array):
    return pltpu.with_memory_space_constraint(array, pltpu.HBM)


def whole(sizes, gate_weight, up_weight, gain, down_weight, tokens, routes, logits):
    nz, ny, nc, nx = sizes
    nyc = ny * nc
    nk = nz * nyc
    per_x = nk // nx
    experts, rows, cols = gate_weight.shape
    width = cols // per_x
    hid, dcols = down_weight.shape[1:]
    bf, f32 = jnp.bfloat16, jnp.float32
    steps = nyc - 1
    sub = rows // PARTS
    count = tokens.shape[0]
    r = count // (nz * ny)
    half = dcols // nc
    dma = pltpu.SemaphoreType.DMA
    vmem = pl.BlockSpec(memory_space=pltpu.VMEM)
    hbm = pl.BlockSpec(memory_space=pltpu.HBM)
    return pl.pallas_call(
        functools.partial(whole_kernel, sizes),
        out_shape=[
            pltpu.VMEM((experts, nz, nyc, rows, width), bf),
            pltpu.VMEM((experts, nz, nyc, rows, width), bf),
            pltpu.VMEM((experts, hid, dcols * nx), bf),
            pltpu.VMEM((count // nk, dcols * nx), bf),
        ],
        in_specs=[hbm, hbm, vmem, hbm, hbm, vmem, vmem],
        out_specs=[vmem] * 4,
        scratch_shapes=[
            pltpu.VMEM(gate_weight.shape, f32),
            pltpu.VMEM(up_weight.shape, f32),
            pltpu.VMEM(down_weight.shape, f32),
            pltpu.VMEM(tokens.shape, bf),
            pltpu.VMEM((2, PARTS, nx, per_x, sub, width), bf),
            pltpu.VMEM((2, PARTS, nk, sub, width), bf),
            pltpu.VMEM((2, PARTS, nz, nyc, sub, width), bf),
            pltpu.VMEM(tokens.shape, bf),
            pltpu.VMEM((experts, count, hid), f32),
            pltpu.VMEM((experts, count, hid), bf),
            pltpu.VMEM((nx, nc, ny, nz, r, half), bf),
            pltpu.VMEM((nx, ny, nz, r, half), bf),
            pltpu.VMEM((nx, ny, nz, r, half), bf),
            pltpu.VMEM((nx, ny, nz, r, half), bf),
            pltpu.VMEM((nx, nz, r, half), bf),
            pltpu.VMEM((nx, nz, r, half), bf),
            pltpu.VMEM((nx, r, half), f32),
            pltpu.VMEM((nx, r // nc, half), f32),
            pltpu.VMEM((nx, r // nc, half), f32),
            dma((4,)),
            dma((2, PARTS, nx)),
            dma((2, PARTS, nx)),
            dma((2, PARTS, nz)),
            dma((2, PARTS, nz)),
            dma((2, PARTS, steps)),
            dma((2, PARTS, steps)),
            dma((2 * PARTS + 1, 2, 2)),
            dma((2 * PARTS + 1, 2, 2)),
            dma((2 * PARTS + 1, 2)),
            dma((2 * PARTS + 1, 2)),
            dma((nx + 1,)),
            dma((nx + 1,)),
            dma((nx, ny)),
            dma((nx, ny)),
            dma((nx, nz)),
            dma((nx, nz)),
        ],
        compiler_params=pltpu.CompilerParams(
            collective_id=0, has_side_effects=True, vmem_limit_bytes=44 * MIB
        ),
        name="whole",
    )(*(away(a) for a in (gate_weight, up_weight)), gain, away(down_weight), away(tokens), routes, logits)


def write_kernel(a, b, c, a_out, b_out, c_out, sems):
    pairs = ((a, a_out), (b, b_out), (c, c_out))
    copies = [pltpu.make_async_copy(src, dst, sems.at[i]) for i, (src, dst) in enumerate(pairs)]
    for copy in copies:
        copy.start()
    for copy in copies:
        copy.wait()


def write_out(*arrays):
    return pl.pallas_call(
        write_kernel,
        out_shape=[jax.ShapeDtypeStruct(a.shape, a.dtype) for a in arrays],
        in_specs=[pl.BlockSpec(memory_space=pltpu.VMEM)] * len(arrays),
        out_specs=[pl.BlockSpec(memory_space=pltpu.HBM)] * len(arrays),
        scratch_shapes=[pltpu.SemaphoreType.DMA((len(arrays),))],
        compiler_params=pltpu.CompilerParams(vmem_limit_bytes=12 * MIB),
        name="write_out",
    )(*arrays)


def shards(sizes, tokens, norm_gain, gate_weight, up_weight, down_weight, routes, route_logit):
    gate, up, down, mixed = whole(
        sizes, gate_weight, up_weight, norm_gain[None, :], down_weight, tokens, routes.T, route_logit.T
    )
    full = (gate.shape[0], -1, gate.shape[-1])
    gate_out, up_out, down_out = write_out(gate.reshape(full), up.reshape(full), down)
    return (gate_out, up_out, down_out, mixed)


def solution(mesh):
    sizes = (8, 4, 2, mesh.shape["tp"])
    finer = Mesh(mesh.devices.reshape(sizes), ("fs_0", "fs_1", "fs_2", "tp"))
    in_specs = (
        P("tp", None),
        P(FS),
        P(None, FS, "tp"),
        P(None, FS, "tp"),
        P(None, FS, "tp"),
        P("tp", None),
        P("tp", None),
    )
    out_specs = (P(None, None, FS), P(None, None, FS), P(None, FS, None), P(TP_FS, None))
    return jax.shard_map(
        functools.partial(shards, sizes),
        mesh=finer,
        in_specs=in_specs,
        out_specs=out_specs,
        check_vma=False,
    )
```

```python
import functools

import jax
import jax.numpy as jnp
from jax import lax
from jax.experimental import pallas as pl
from jax.experimental.pallas import tpu as pltpu
from jax.sharding import Mesh
from jax.sharding import PartitionSpec as P

FS = ("fs_0", "fs_1", "fs_2")
TP_FS = ("tp", "fs_0", "fs_1", "fs_2")
EPS = 0.5
MESH = pl.DeviceIdType.MESH
MIB = 1024 * 1024
SPLIT = 1
DIRECT = ()
PARTS = 2


def whole_kernel(
    sizes,
    gate_hbm,
    up_hbm,
    gain_hbm,
    down_hbm,
    token_hbm,
    route_hbm,
    logit_hbm,
    gate_out,
    up_out,
    down_out,
    mixed_out,
    gate_in,
    up_in,
    down_in,
    token_in,
    gain_ref,
    route_ref,
    logit_ref,
    staged,
    spread,
    by_z,
    normed,
    share,
    hidden,
    part,
    from_twin,
    to_y,
    from_y,
    far_in,
    of_y,
    to_z,
    from_z,
    total,
    other,
    last,
    in_sem,
    a_send,
    a_recv,
    z_send,
    z_recv,
    y_send,
    y_recv,
    c_send,
    c_recv,
    f_send,
    f_recv,
    t_send,
    t_recv,
    ry_send,
    ry_recv,
    rz_send,
    rz_recv,
):
    nz, ny, nc, nx = sizes
    nyc = ny * nc
    nk = nz * nyc
    per_x = nk // nx
    f32, bf = jnp.float32, jnp.bfloat16
    my_z, my_y = lax.axis_index("fs_0"), lax.axis_index("fs_1")
    my_c, my_x = lax.axis_index("fs_2"), lax.axis_index("tp")
    my_yc = my_y * nc + my_c
    outs = (gate_out, up_out)

    loads = [
        pltpu.make_async_copy(src, dst, in_sem.at[i])
        for i, (src, dst) in enumerate(
            (
                (gate_hbm, gate_in),
                (up_hbm, up_in),
                (down_hbm, down_in),
                (token_hbm, token_in),
                (gain_hbm, gain_ref),
                (route_hbm, route_ref),
                (logit_hbm, logit_ref),
            )
        )
    ]
    for i in (4, 0, 1, 2, 5, 6, 3):
        loads[i].start()

    def at(dz=0, dy=0, dc=0, dx=0):
        return (
            lax.rem(my_z + dz, nz),
            lax.rem(my_y + dy, ny),
            lax.rem(my_c + dc, nc),
            lax.rem(my_x + dx, nx),
        )

    yc_steps = [(dy, dc) for dy in range(ny) for dc in range(nc) if dy + dc > 0]
    peers = (
        [at(dx=d) for d in range(1, nx)]
        + [at(dz=d) for d in range(1, nz)]
        + [at(dy=dy, dc=dc) for dy, dc in yc_steps]
    )
    barrier = pltpu.get_barrier_semaphore()
    for peer in peers:
        pl.semaphore_signal(barrier, inc=1, device_id=peer, device_id_type=MESH)

    sent = []

    def start(src, dst, ssem, rsem, peer):
        copy = pltpu.make_async_remote_copy(
            src_ref=src, dst_ref=dst, send_sem=ssem, recv_sem=rsem, device_id=peer, device_id_type=MESH
        )
        copy.start()
        sent.append(copy)
        return copy

    rows = gate_in.shape[1]
    width = gate_in.shape[2] // per_x
    sub = rows // PARTS
    loads[4].wait()
    gain_row = gain_ref[...]
    same = lax.broadcasted_iota(jnp.int32, (rows, rows), 0) == lax.broadcasted_iota(
        jnp.int32, (rows, rows), 1
    )
    gain = jnp.sum(jnp.where(same, gain_row, 0.0), axis=1, keepdims=True)
    chunks = [(m, h) for m in (0, 1) for h in range(PARTS)]

    a_copies = {}
    for m, ref in ((0, gate_in), (1, up_in)):
        loads[m].wait()
        for h in range(PARTS):
            lo = h * sub
            for d in range(nx):
                expert = lax.rem(my_x + d, nx)
                for k in range(per_x):
                    block = ref[expert, lo : lo + sub, k * width : (k + 1) * width]
                    block = (block * gain[lo : lo + sub]).astype(bf)
                    if d == 0:
                        spread[m, h, my_x * per_x + k] = block
                    else:
                        staged[m, h, d, k] = block
            if m + h == 0:
                pl.semaphore_wait(barrier, len(peers))
            for d in range(1, nx):
                a_copies[m, h, d] = start(
                    staged.at[m, h, d],
                    spread.at[m, h, pl.ds(my_x * per_x, per_x)],
                    a_send.at[m, h, d],
                    a_recv.at[m, h, d],
                    at(dx=d),
                )

    cols = down_in.shape[2]
    half_e = nx // 2
    loads[2].wait()
    own_cols = pl.ds(pl.multiple_of(my_x * cols, cols), cols)
    for e in range(nx):
        down_out[e, :, own_cols] = down_in[e].astype(bf)

    left, right = lax.rem(my_x + nx - 1, nx), lax.rem(my_x + 1, nx)

    def near(tag, block, side, h):
        ref = block(my_x, h)
        return start(
            ref, ref, c_send.at[tag, side, h], c_recv.at[tag, side, h], at(dx=1 if side == 0 else nx - 1)
        )

    def pass_on(tag, block, side):
        ref = block(left if side == 0 else right, side)
        return start(
            ref, ref, f_send.at[tag, side], f_recv.at[tag, side], at(dx=1 if side == 0 else nx - 1)
        )

    def down_block(x, h):
        return down_out.at[
            pl.ds(h * half_e, half_e), :, pl.ds(pl.multiple_of(x * cols, cols), cols)
        ]

    d_tag = len(chunks)
    d_near = {}
    for s in (0, 1):
        d_near[s, s] = near(d_tag, down_block, s, s)
    for s in (0, 1):
        d_near[s, 1 - s] = near(d_tag, down_block, s, 1 - s)

    loads[3].wait()
    step = 48

    def norm_rows(i, carry):
        at_rows = pl.ds(pl.multiple_of(i * step, step), step)
        floats = token_in[at_rows, :].astype(f32)
        scale = lax.rsqrt(jnp.mean(floats * floats, axis=1, keepdims=True) + EPS)
        normed[at_rows, :] = (floats * scale).astype(bf)
        return carry

    lax.fori_loop(0, token_in.shape[0] // step, norm_rows, 0)
    loads[5].wait()
    loads[6].wait()
    first = 1.0 / (1.0 + jnp.exp(logit_ref[1:2, :] - logit_ref[0:1, :]))
    lines = [
        jnp.where(route_ref[0:1, :] == e, first, 0.0)
        + jnp.where(route_ref[1:2, :] == e, 1.0 - first, 0.0)
        for e in range(nx)
    ]
    lines.append(jnp.zeros((128 - nx, first.shape[1]), f32))
    columns = jnp.concatenate(lines, axis=0).T
    for e in range(nx):
        share[e] = jnp.broadcast_to(columns[:, e : e + 1], share.shape[1:])

    z_copies, y_copies, c_near, c_far = {}, {}, {}, {}
    half_z = nz // 2

    def over_z(q):
        m, h = q
        for d in range(1, nx):
            a_copies[m, h, d].wait_recv()
        for dz in range(1, nz):
            peer = at(dz=dz)
            z_copies[q, dz] = start(
                spread.at[m, h, pl.ds(peer[0] * nyc, nyc)],
                by_z.at[m, h, my_z],
                z_send.at[m, h, dz],
                z_recv.at[m, h, dz],
                peer,
            )
        by_z[m, h, my_z] = spread[m, h, pl.ds(my_z * nyc, nyc)]

    def over_yc(q):
        m, h = q
        out, lo = outs[m], h * sub
        for dz in range(1, nz):
            z_copies[q, dz].wait_recv()
        for i, (dy, dc) in enumerate(yc_steps):
            peer = at(dy=dy, dc=dc)
            y_copies[q, i] = start(
                by_z.at[m, h, :, peer[1] * nc + peer[2]],
                out.at[my_x, :, my_yc, pl.ds(lo, sub)],
                y_send.at[m, h, i],
                y_recv.at[m, h, i],
                peer,
            )
        out[my_x, :, my_yc, lo : lo + sub, :] = by_z[m, h, :, my_yc]

    def out_block(q):
        m, h = q
        return lambda x, half: outs[m].at[x, pl.ds(half * half_z, half_z), :, pl.ds(h * sub, sub)]

    def over_x(q):
        tag = chunks.index(q)
        for i in range(len(yc_steps)):
            y_copies[q, i].wait_recv()
        for s in (0, 1):
            c_near[q, s, s] = near(tag, out_block(q), s, s)
        for s in (0, 1):
            c_near[q, s, 1 - s] = near(tag, out_block(q), s, 1 - s)

    def onward(q):
        for s in (0, 1):
            c_near[q, s, s].wait_recv()
            c_far[q, s] = pass_on(chunks.index(q), out_block(q), s)

    experts = nx
    hid = width
    tiles = 2
    tile_rows = normed.shape[0] // tiles
    z_per = nz // tiles
    r = normed.shape[0] // (nz * ny)

    def run_expert(e):
        def tile(t, carry):
            at_rows = pl.ds(pl.multiple_of(t * tile_rows, tile_rows), tile_rows)
            shape = (nk * rows, width)
            both = jnp.concatenate([gate_out[e].reshape(shape), up_out[e].reshape(shape)], axis=1)
            val = jnp.dot(normed[at_rows, :], both, preferred_element_type=f32)
            gate_val, up_val = val[:, :hid], val[:, hid:]
            weight = share[e, at_rows, :]
            value = gate_val / (1.0 + jnp.exp(-gate_val)) * up_val
            hidden[e, at_rows, :] = jnp.where(weight > 0.0, value * weight, 0.0).astype(bf)
            return carry

        lax.fori_loop(0, tiles, tile, 0)

    q0, q1, q2, q3 = chunks
    over_z(q0)
    over_z(q1)
    over_z(q2)
    over_yc(q0)
    over_z(q3)
    over_x(q0)
    over_yc(q1)
    onward(q0)
    over_x(q1)
    over_yc(q2)
    onward(q1)
    over_x(q2)
    over_yc(q3)
    onward(q2)
    over_x(q3)
    run_expert(my_x)
    onward(q3)
    d_far = []
    for s in (0, 1):
        d_near[s, s].wait_recv()
        d_far.append(pass_on(d_tag, down_block, s))
    for s, e in ((0, left), (1, right)):
        for q in chunks:
            c_near[q, s, 1 - s].wait_recv()
        run_expert(e)
    for q in chunks:
        for s in (0, 1):
            c_far[q, s].wait_recv()
    run_expert(lax.rem(my_x + nx // 2, nx))

    piece = cols // SPLIT
    half = piece // nc
    twin = at(dc=1)
    y_peers = [at(dy=d) for d in range(ny)]
    z_peers = [at(dz=d) for d in range(nz)]
    owners = [my_x, left, right, lax.rem(my_x + nx // 2, nx)]
    blocks = [(x, i * piece) for x in owners for i in range(SPLIT)]
    twin_copies, sum_y_copies, sum_z_copies = {}, {}, {}

    def multiply(b):
        x, offset = blocks[b]
        at_cols = pl.ds(pl.multiple_of(x * cols + offset, piece), piece)

        def tile(t, carry):
            at_rows = pl.ds(pl.multiple_of(t * tile_rows, tile_rows), tile_rows)
            units = jnp.concatenate([hidden[e, at_rows, :] for e in range(experts)], axis=1)
            down = down_out[:, :, at_cols].reshape(experts * hid, piece)
            val = jnp.dot(units, down, preferred_element_type=f32)
            val = val.reshape(z_per, ny, r, piece)
            at_part = pl.ds(pl.multiple_of(t * z_per * r, z_per * r), z_per * r)
            for y in range(ny):
                lines = jnp.concatenate([val[z, y] for z in range(z_per)], axis=0).astype(bf)
                for c in range(nc):
                    part[b, c, y, at_part, :] = lines[:, c * half : (c + 1) * half]
            return carry

        lax.fori_loop(0, tiles, tile, 0)
        twin_copies[b] = start(
            part.at[b, twin[2]], from_twin.at[b], t_send.at[b], t_recv.at[b], twin
        )

    far_y = ny // 2
    count_y = nz * r
    halves = (pl.ds(0, count_y // 2), pl.ds(count_y // 2, count_y // 2))

    def to_y_send(b, lane, part_of, landing, target):
        sum_y_copies[b, lane] = start(
            part_of, landing, ry_send.at[b, lane], ry_recv.at[b, lane], target
        )

    def pair_sum(b, y, where):
        return part[b, my_c, y, where, :] + from_twin[b, y, where, :]

    def sum_over_y(b):
        twin_copies[b].wait_recv()
        right_y, far, left_y = (y_peers[d][1] for d in (1, far_y, ny - 1))
        for lane, side in ((0, 1), (1, ny - 1)):
            to_y[b, far, halves[lane], :] = pair_sum(b, far, halves[lane])
            to_y_send(
                b, lane, to_y.at[b, far, halves[lane]], far_in.at[b, lane], y_peers[side]
            )
        for lane, side, near_y, where in (
            (2, 1, right_y, halves[1]),
            (3, ny - 1, left_y, halves[0]),
        ):
            to_y[b, near_y, where, :] = pair_sum(b, near_y, where)
            to_y_send(
                b, lane, to_y.at[b, near_y, where], from_y.at[b, lane - 2, where], y_peers[side]
            )

    def direct_y(b):
        twin_copies[b].wait_recv()
        for d in (far_y, 1, ny - 1):
            y = y_peers[d][1]
            to_y[b, y] = pair_sum(b, y, slice(None))
            to_y_send(b, d, to_y.at[b, y], from_y.at[b, d - 1], y_peers[d])

    def relay_y(b):
        right_y, left_y = y_peers[1][1], y_peers[ny - 1][1]
        for lane, side, near_y, where, came in (
            (4, 1, right_y, halves[0], 0),
            (5, ny - 1, left_y, halves[1], 1),
        ):
            sum_y_copies[b, came].wait_recv()
            to_y[b, near_y, where, :] = pair_sum(b, near_y, where) + far_in[b, came]
            to_y_send(
                b, lane, to_y.at[b, near_y, where], from_y.at[b, lane - 4, where], y_peers[side]
            )

    def sum_over_z(b):
        for lane in range(1, ny) if b in DIRECT else range(2, 6):
            sum_y_copies[b, lane].wait_recv()
        value = part[b, my_c, my_y].astype(f32) + from_twin[b, my_y].astype(f32)
        for side in range(ny - 1 if b in DIRECT else 2):
            value = value + from_y[b, side].astype(f32)
        value = value.reshape(nz, r, half)
        of_y[b] = value
        to_z[b] = value.astype(bf)
        for d in range(1, nz):
            sum_z_copies[b, d] = start(
                to_z.at[b, z_peers[d][0]],
                from_z.at[b, d],
                rz_send.at[b, d],
                rz_recv.at[b, d],
                z_peers[d],
            )

    def finish(b):
        value = of_y[b, my_z]
        for d in range(1, nz):
            sum_z_copies[b, d].wait_recv()
            value = value + from_z[b, d].astype(f32)
        total[b] = value

    count = len(blocks)

    def first_y(b):
        (direct_y if b in DIRECT else sum_over_y)(b)

    def second_y(b):
        if b not in DIRECT:
            relay_y(b)

    for i in range(count + 5):
        if i == SPLIT:
            d_near[0, 1].wait_recv()
        if i == 2 * SPLIT:
            d_near[1, 0].wait_recv()
        if i == 3 * SPLIT:
            for copy in d_far:
                copy.wait_recv()
        for stage, lag in ((multiply, 0), (first_y, 1), (second_y, 2), (sum_over_z, 3), (finish, 5)):
            if 0 <= i - lag < count:
                stage(i - lag)

    own = mixed_out.shape[0]
    first_core = my_c == 0
    low, high = total[:, 0:own, :], total[:, own : 2 * own, :]
    other[...] = jnp.where(first_core, high, low)
    swap = start(other, last, t_send.at[len(blocks)], t_recv.at[len(blocks)], twin)
    mine = jnp.where(first_core, low, high)
    swap.wait_recv()
    theirs = last[...]
    for b, (x, offset) in enumerate(blocks):
        pair = [
            jnp.where(first_core, mine[b], theirs[b]),
            jnp.where(first_core, theirs[b], mine[b]),
        ]
        at_cols = pl.ds(pl.multiple_of(x * cols + offset, piece), piece)
        mixed_out[:, at_cols] = jnp.concatenate(pair, axis=1).astype(bf)
    for copy in sent:
        copy.wait_send()


def away(array):
    return pltpu.with_memory_space_constraint(array, pltpu.HBM)


def whole(sizes, gate_weight, up_weight, gain, down_weight, tokens, routes, logits):
    nz, ny, nc, nx = sizes
    nyc = ny * nc
    nk = nz * nyc
    per_x = nk // nx
    experts, rows, cols = gate_weight.shape
    width = cols // per_x
    hid, dcols = down_weight.shape[1:]
    bf, f32 = jnp.bfloat16, jnp.float32
    steps = nyc - 1
    sub = rows // PARTS
    count = tokens.shape[0]
    r = count // (nz * ny)
    nb = nx * SPLIT
    half = dcols // nc // SPLIT
    dma = pltpu.SemaphoreType.DMA
    vmem = pl.BlockSpec(memory_space=pltpu.VMEM)
    hbm = pl.BlockSpec(memory_space=pltpu.HBM)
    return pl.pallas_call(
        functools.partial(whole_kernel, sizes),
        out_shape=[
            pltpu.VMEM((experts, nz, nyc, rows, width), bf),
            pltpu.VMEM((experts, nz, nyc, rows, width), bf),
            pltpu.VMEM((experts, hid, dcols * nx), bf),
            pltpu.VMEM((count // nk, dcols * nx), bf),
        ],
        in_specs=[hbm] * 7,
        out_specs=[vmem] * 4,
        scratch_shapes=[
            pltpu.VMEM(gate_weight.shape, f32),
            pltpu.VMEM(up_weight.shape, f32),
            pltpu.VMEM(down_weight.shape, f32),
            pltpu.VMEM(tokens.shape, bf),
            pltpu.VMEM(gain.shape, f32),
            pltpu.VMEM(routes.shape, jnp.int32),
            pltpu.VMEM(logits.shape, f32),
            pltpu.VMEM((2, PARTS, nx, per_x, sub, width), bf),
            pltpu.VMEM((2, PARTS, nk, sub, width), bf),
            pltpu.VMEM((2, PARTS, nz, nyc, sub, width), bf),
            pltpu.VMEM(tokens.shape, bf),
            pltpu.VMEM((experts, count, hid), f32),
            pltpu.VMEM((experts, count, hid), bf),
            pltpu.VMEM((nb, nc, ny, nz * r, half), bf),
            pltpu.VMEM((nb, ny, nz * r, half), bf),
            pltpu.VMEM((nb, ny, nz * r, half), bf),
            pltpu.VMEM((nb, ny - 1, nz * r, half), bf),
            pltpu.VMEM((nb, 2, nz * r // 2, half), bf),
            pltpu.VMEM((nb, nz, r, half), f32),
            pltpu.VMEM((nb, nz, r, half), bf),
            pltpu.VMEM((nb, nz, r, half), bf),
            pltpu.VMEM((nb, r, half), f32),
            pltpu.VMEM((nb, r // nc, half), f32),
            pltpu.VMEM((nb, r // nc, half), f32),
            dma((7,)),
            dma((2, PARTS, nx)),
            dma((2, PARTS, nx)),
            dma((2, PARTS, nz)),
            dma((2, PARTS, nz)),
            dma((2, PARTS, steps)),
            dma((2, PARTS, steps)),
            dma((2 * PARTS + 1, 2, 2)),
            dma((2 * PARTS + 1, 2, 2)),
            dma((2 * PARTS + 1, 2)),
            dma((2 * PARTS + 1, 2)),
            dma((nb + 1,)),
            dma((nb + 1,)),
            dma((nb, 6)),
            dma((nb, 6)),
            dma((nb, nz)),
            dma((nb, nz)),
        ],
        compiler_params=pltpu.CompilerParams(
            collective_id=0, has_side_effects=True, vmem_limit_bytes=44 * MIB
        ),
        name="whole",
    )(*(away(a) for a in (gate_weight, up_weight, gain, down_weight, tokens, routes, logits)))


def write_kernel(*refs):
    count = len(refs) // 2
    copies = [
        pltpu.make_async_copy(refs[i], refs[count + i], refs[-1].at[i]) for i in range(count)
    ]
    for copy in copies:
        copy.start()
    for copy in copies:
        copy.wait()


def write_out(*arrays):
    return pl.pallas_call(
        write_kernel,
        out_shape=[jax.ShapeDtypeStruct(a.shape, a.dtype) for a in arrays],
        in_specs=[pl.BlockSpec(memory_space=pltpu.VMEM)] * len(arrays),
        out_specs=[pl.BlockSpec(memory_space=pltpu.HBM)] * len(arrays),
        scratch_shapes=[pltpu.SemaphoreType.DMA((len(arrays),))],
        compiler_params=pltpu.CompilerParams(vmem_limit_bytes=12 * MIB),
        name="write_out",
    )(*arrays)


def shards(sizes, tokens, norm_gain, gate_weight, up_weight, down_weight, routes, route_logit):
    gate, up, down, mixed = whole(
        sizes, gate_weight, up_weight, norm_gain[None, :], down_weight, tokens, routes.T, route_logit.T
    )
    full = (gate.shape[0], -1, gate.shape[-1])
    return tuple(write_out(gate.reshape(full), up.reshape(full), down, mixed))


def solution(mesh):
    sizes = (8, 4, 2, mesh.shape["tp"])
    finer = Mesh(mesh.devices.reshape(sizes), ("fs_0", "fs_1", "fs_2", "tp"))
    in_specs = (
        P("tp", None),
        P(FS),
        P(None, FS, "tp"),
        P(None, FS, "tp"),
        P(None, FS, "tp"),
        P("tp", None),
        P("tp", None),
    )
    out_specs = (P(None, None, FS), P(None, None, FS), P(None, FS, None), P(TP_FS, None))
    return jax.shard_map(
        functools.partial(shards, sizes),
        mesh=finer,
        in_specs=in_specs,
        out_specs=out_specs,
        check_vma=False,
    )
```

```python
import functools

import jax
import jax.numpy as jnp
from jax import lax
from jax.experimental import pallas as pl
from jax.experimental.pallas import tpu as pltpu
from jax.sharding import Mesh
from jax.sharding import PartitionSpec as P

FS = ("fs_0", "fs_1", "fs_2")
TP_FS = ("tp", "fs_0", "fs_1", "fs_2")
EPS = 0.5
MESH = pl.DeviceIdType.MESH
MIB = 1024 * 1024
SPLIT = 1
DIRECT = (3,)


def whole_kernel(
    sizes,
    gate_hbm,
    up_hbm,
    gain_hbm,
    down_hbm,
    token_hbm,
    route_hbm,
    logit_hbm,
    gate_out,
    up_out,
    down_out,
    mixed_out,
    gate_in,
    up_in,
    down_in,
    token_in,
    gain_ref,
    route_ref,
    logit_ref,
    staged,
    spread,
    by_z,
    staged_b,
    spread_b,
    by_z_b,
    wide,
    wide_by_z,
    normed,
    share,
    hidden,
    part,
    from_twin,
    to_y,
    from_y,
    far_in,
    of_y,
    to_z,
    from_z,
    total,
    other,
    last,
    in_sem,
    a_send,
    a_recv,
    z_send,
    z_recv,
    wz_send,
    wz_recv,
    wy_send,
    wy_recv,
    y_send,
    y_recv,
    c_send,
    c_recv,
    f_send,
    f_recv,
    t_send,
    t_recv,
    ry_send,
    ry_recv,
    rz_send,
    rz_recv,
):
    nz, ny, nc, nx = sizes
    nyc = ny * nc
    nk = nz * nyc
    per_x = nk // nx
    f32, bf = jnp.float32, jnp.bfloat16
    my_z, my_y = lax.axis_index("fs_0"), lax.axis_index("fs_1")
    my_c, my_x = lax.axis_index("fs_2"), lax.axis_index("tp")
    my_yc = my_y * nc + my_c
    outs = (gate_out, up_out)

    loads = [
        pltpu.make_async_copy(src, dst, in_sem.at[i])
        for i, (src, dst) in enumerate(
            (
                (gate_hbm, gate_in),
                (up_hbm, up_in),
                (down_hbm, down_in),
                (token_hbm, token_in),
                (gain_hbm, gain_ref),
                (route_hbm, route_ref),
                (logit_hbm, logit_ref),
            )
        )
    ]
    for i in (4, 0, 1, 2, 5, 6, 3):
        loads[i].start()

    def at(dz=0, dy=0, dc=0, dx=0):
        return (
            lax.rem(my_z + dz, nz),
            lax.rem(my_y + dy, ny),
            lax.rem(my_c + dc, nc),
            lax.rem(my_x + dx, nx),
        )

    yc_steps = [(dy, dc) for dy in range(ny) for dc in range(nc) if dy + dc > 0]
    peers = (
        [at(dx=d) for d in range(1, nx)]
        + [at(dz=d) for d in range(1, nz)]
        + [at(dy=dy, dc=dc) for dy, dc in yc_steps]
    )
    barrier = pltpu.get_barrier_semaphore()
    for peer in peers:
        pl.semaphore_signal(barrier, inc=1, device_id=peer, device_id_type=MESH)

    sent = []

    def start(src, dst, ssem, rsem, peer):
        copy = pltpu.make_async_remote_copy(
            src_ref=src, dst_ref=dst, send_sem=ssem, recv_sem=rsem, device_id=peer, device_id_type=MESH
        )
        copy.start()
        sent.append(copy)
        return copy

    rows = gate_in.shape[1]
    width = gate_in.shape[2] // per_x
    loads[4].wait()
    gain_row = gain_ref[...]
    same = lax.broadcasted_iota(jnp.int32, (rows, rows), 0) == lax.broadcasted_iota(
        jnp.int32, (rows, rows), 1
    )
    gain = jnp.sum(jnp.where(same, gain_row, 0.0), axis=1, keepdims=True)
    step_a, step_b = rows // 2, rows // 4
    chunks = [
        (0, 0, step_a),
        (0, step_a, step_a),
        (1, 0, step_a),
        (1, step_a, step_b),
        (1, step_a + step_b, step_b),
    ]
    stages = [(staged.at[i], spread.at[i], by_z.at[i]) for i in range(3)]
    stages.append((staged_b, spread_b, by_z_b))

    a_copies = {}
    for q, (m, lo, n) in enumerate(chunks):
        ref = (gate_in, up_in)[m]
        if lo == 0:
            loads[m].wait()
        for d in range(nx):
            expert = lax.rem(my_x + d, nx)
            for k in range(per_x):
                block = ref[expert, lo : lo + n, k * width : (k + 1) * width]
                block = (block * gain[lo : lo + n]).astype(bf)
                if q == len(chunks) - 1:
                    wide[expert, my_x * per_x + k] = block
                elif d == 0:
                    stages[q][1][my_x * per_x + k] = block
                else:
                    stages[q][0][d, k] = block
        if q == 0:
            pl.semaphore_wait(barrier, len(peers))
        if q == len(chunks) - 1:
            continue
        for d in range(1, nx):
            a_copies[q, d] = start(
                stages[q][0].at[d],
                stages[q][1].at[pl.ds(my_x * per_x, per_x)],
                a_send.at[q, d],
                a_recv.at[q, d],
                at(dx=d),
            )

    cols = down_in.shape[2]
    half_e = nx // 2
    loads[2].wait()
    own_cols = pl.ds(pl.multiple_of(my_x * cols, cols), cols)
    for e in range(nx):
        down_out[e, :, own_cols] = down_in[e].astype(bf)

    left, right = lax.rem(my_x + nx - 1, nx), lax.rem(my_x + 1, nx)

    def near(tag, block, side, h):
        ref = block(my_x, h)
        return start(
            ref, ref, c_send.at[tag, side, h], c_recv.at[tag, side, h], at(dx=1 if side == 0 else nx - 1)
        )

    def pass_on(tag, block, side):
        ref = block(left if side == 0 else right, side)
        return start(
            ref, ref, f_send.at[tag, side], f_recv.at[tag, side], at(dx=1 if side == 0 else nx - 1)
        )

    def down_block(x, h):
        return down_out.at[
            pl.ds(h * half_e, half_e), :, pl.ds(pl.multiple_of(x * cols, cols), cols)
        ]

    def near_all(tag, block):
        copies = {(s, s): near(tag, block, s, s) for s in (0, 1)}
        copies.update({(s, 1 - s): near(tag, block, s, 1 - s) for s in (0, 1)})
        return copies

    def wide_block(x, h):
        return wide.at[
            pl.ds(h * half_e, half_e), pl.ds(pl.multiple_of(x * per_x, per_x), per_x)
        ]

    w_tag, d_tag = len(chunks) - 1, len(chunks)
    w_near = near_all(w_tag, wide_block)

    loads[3].wait()
    step = 48

    def norm_rows(i, carry):
        at_rows = pl.ds(pl.multiple_of(i * step, step), step)
        floats = token_in[at_rows, :].astype(f32)
        scale = lax.rsqrt(jnp.mean(floats * floats, axis=1, keepdims=True) + EPS)
        normed[at_rows, :] = (floats * scale).astype(bf)
        return carry

    lax.fori_loop(0, token_in.shape[0] // step, norm_rows, 0)
    loads[5].wait()
    loads[6].wait()
    first = 1.0 / (1.0 + jnp.exp(logit_ref[1:2, :] - logit_ref[0:1, :]))
    lines = [
        jnp.where(route_ref[0:1, :] == e, first, 0.0)
        + jnp.where(route_ref[1:2, :] == e, 1.0 - first, 0.0)
        for e in range(nx)
    ]
    lines.append(jnp.zeros((128 - nx, first.shape[1]), f32))
    columns = jnp.concatenate(lines, axis=0).T
    for e in range(nx):
        share[e] = jnp.broadcast_to(columns[:, e : e + 1], share.shape[1:])

    z_copies, y_copies, c_near, c_far = {}, {}, {}, {}
    half_z = nz // 2

    def over_z(q):
        _, by_x, by_z_q = stages[q]
        for d in range(1, nx):
            a_copies[q, d].wait_recv()
        for dz in range(1, nz):
            peer = at(dz=dz)
            z_copies[q, dz] = start(
                by_x.at[pl.ds(peer[0] * nyc, nyc)],
                by_z_q.at[my_z],
                z_send.at[q, dz],
                z_recv.at[q, dz],
                peer,
            )
        by_z_q[my_z] = by_x[pl.ds(my_z * nyc, nyc)]

    def over_yc(q):
        m, lo, n = chunks[q]
        out, by_z_q = outs[m], stages[q][2]
        for dz in range(1, nz):
            z_copies[q, dz].wait_recv()
        for i, (dy, dc) in enumerate(yc_steps):
            peer = at(dy=dy, dc=dc)
            y_copies[q, i] = start(
                by_z_q.at[:, peer[1] * nc + peer[2]],
                out.at[my_x, :, my_yc, pl.ds(lo, n)],
                y_send.at[q, i],
                y_recv.at[q, i],
                peer,
            )
        out[my_x, :, my_yc, lo : lo + n, :] = by_z_q[:, my_yc]

    def out_block(q):
        m, lo, n = chunks[q]
        return lambda x, half: outs[m].at[x, pl.ds(half * half_z, half_z), :, pl.ds(lo, n)]

    def over_x(q):
        tag = q
        for i in range(len(yc_steps)):
            y_copies[q, i].wait_recv()
        for s in (0, 1):
            c_near[q, s, s] = near(tag, out_block(q), s, s)
        for s in (0, 1):
            c_near[q, s, 1 - s] = near(tag, out_block(q), s, 1 - s)

    def onward(q):
        for s in (0, 1):
            c_near[q, s, s].wait_recv()
            c_far[q, s] = pass_on(q, out_block(q), s)

    experts = nx
    hid = width
    tiles = 2
    tile_rows = normed.shape[0] // tiles
    z_per = nz // tiles
    r = normed.shape[0] // (nz * ny)

    def run_expert(e):
        def tile(t, carry):
            at_rows = pl.ds(pl.multiple_of(t * tile_rows, tile_rows), tile_rows)
            shape = (nk * rows, width)
            both = jnp.concatenate([gate_out[e].reshape(shape), up_out[e].reshape(shape)], axis=1)
            val = jnp.dot(normed[at_rows, :], both, preferred_element_type=f32)
            gate_val, up_val = val[:, :hid], val[:, hid:]
            weight = share[e, at_rows, :]
            value = gate_val / (1.0 + jnp.exp(-gate_val)) * up_val
            hidden[e, at_rows, :] = jnp.where(weight > 0.0, value * weight, 0.0).astype(bf)
            return carry

        lax.fori_loop(0, tiles, tile, 0)

    order = [my_x, left, right, lax.rem(my_x + nx // 2, nx)]
    w_out, w_lo, sub = outs[chunks[-1][0]], chunks[-1][1], chunks[-1][2]
    wz_copies, wy_copies = {}, {}

    def wide_over_z():
        for s in (0, 1):
            w_near[s, 1 - s].wait_recv()
        for copy in w_onward:
            copy.wait_recv()
        for i, e in enumerate(order):
            for dz in range(1, nz):
                peer = at(dz=dz)
                wz_copies[i, dz] = start(
                    wide.at[e, pl.ds(peer[0] * nyc, nyc)],
                    wide_by_z.at[e, my_z],
                    wz_send.at[i, dz],
                    wz_recv.at[i, dz],
                    peer,
                )
            wide_by_z[e, my_z] = wide[e, pl.ds(my_z * nyc, nyc)]

    def wide_over_yc(i):
        e = order[i]
        for dz in range(1, nz):
            wz_copies[i, dz].wait_recv()
        for j, (dy, dc) in enumerate(yc_steps):
            peer = at(dy=dy, dc=dc)
            wy_copies[i, j] = start(
                wide_by_z.at[e, :, peer[1] * nc + peer[2]],
                w_out.at[e, :, my_yc, pl.ds(w_lo, sub)],
                wy_send.at[i, j],
                wy_recv.at[i, j],
                peer,
            )
        w_out[e, :, my_yc, w_lo : w_lo + sub, :] = wide_by_z[e, :, my_yc]

    def wide_done(i):
        for j in range(len(yc_steps)):
            wy_copies[i, j].wait_recv()

    over_z(0)
    over_z(1)
    over_z(2)
    over_yc(0)
    over_z(3)
    w_onward = []
    for s in (0, 1):
        w_near[s, s].wait_recv()
        w_onward.append(pass_on(w_tag, wide_block, s))
    d_near = {(s, s): near(d_tag, down_block, s, s) for s in (0, 1)}
    over_x(0)
    over_yc(1)
    wide_over_z()
    over_yc(2)
    over_x(1)
    onward(0)
    over_yc(3)
    over_x(2)
    wide_over_yc(0)
    over_x(3)
    onward(1)
    wide_over_yc(1)
    wide_done(0)
    run_expert(order[0])
    wide_over_yc(2)
    wide_over_yc(3)
    onward(2)
    onward(3)
    for s in (0, 1):
        d_near[s, 1 - s] = near(d_tag, down_block, s, 1 - s)
    d_far = []
    for s in (0, 1):
        d_near[s, s].wait_recv()
        d_far.append(pass_on(d_tag, down_block, s))
    for i, s in ((1, 0), (2, 1)):
        wide_done(i)
        for q in range(4):
            c_near[q, s, 1 - s].wait_recv()
        run_expert(order[i])
    wide_done(3)
    for q in range(4):
        for s in (0, 1):
            c_far[q, s].wait_recv()
    run_expert(order[3])

    piece = cols // SPLIT
    half = piece // nc
    twin = at(dc=1)
    y_peers = [at(dy=d) for d in range(ny)]
    z_peers = [at(dz=d) for d in range(nz)]
    owners = [my_x, left, right, lax.rem(my_x + nx // 2, nx)]
    blocks = [(x, i * piece) for x in owners for i in range(SPLIT)]
    twin_copies, sum_y_copies, sum_z_copies = {}, {}, {}

    def multiply(b):
        x, offset = blocks[b]
        at_cols = pl.ds(pl.multiple_of(x * cols + offset, piece), piece)

        def tile(t, carry):
            at_rows = pl.ds(pl.multiple_of(t * tile_rows, tile_rows), tile_rows)
            units = jnp.concatenate([hidden[e, at_rows, :] for e in range(experts)], axis=1)
            down = down_out[:, :, at_cols].reshape(experts * hid, piece)
            val = jnp.dot(units, down, preferred_element_type=f32)
            val = val.reshape(z_per, ny, r, piece)
            at_part = pl.ds(pl.multiple_of(t * z_per * r, z_per * r), z_per * r)
            for y in range(ny):
                lines = jnp.concatenate([val[z, y] for z in range(z_per)], axis=0).astype(bf)
                for c in range(nc):
                    part[b, c, y, at_part, :] = lines[:, c * half : (c + 1) * half]
            return carry

        lax.fori_loop(0, tiles, tile, 0)
        twin_copies[b] = start(
            part.at[b, twin[2]], from_twin.at[b], t_send.at[b], t_recv.at[b], twin
        )

    far_y = ny // 2
    count_y = nz * r
    halves = (pl.ds(0, count_y // 2), pl.ds(count_y // 2, count_y // 2))

    def to_y_send(b, lane, part_of, landing, target):
        sum_y_copies[b, lane] = start(
            part_of, landing, ry_send.at[b, lane], ry_recv.at[b, lane], target
        )

    def pair_sum(b, y, where):
        return part[b, my_c, y, where, :] + from_twin[b, y, where, :]

    def sum_over_y(b):
        twin_copies[b].wait_recv()
        right_y, far, left_y = (y_peers[d][1] for d in (1, far_y, ny - 1))
        for lane, side in ((0, 1), (1, ny - 1)):
            to_y[b, far, halves[lane], :] = pair_sum(b, far, halves[lane])
            to_y_send(
                b, lane, to_y.at[b, far, halves[lane]], far_in.at[b, lane], y_peers[side]
            )
        for lane, side, near_y, where in (
            (2, 1, right_y, halves[1]),
            (3, ny - 1, left_y, halves[0]),
        ):
            to_y[b, near_y, where, :] = pair_sum(b, near_y, where)
            to_y_send(
                b, lane, to_y.at[b, near_y, where], from_y.at[b, lane - 2, where], y_peers[side]
            )

    def direct_y(b):
        twin_copies[b].wait_recv()
        for d in (far_y, 1, ny - 1):
            y = y_peers[d][1]
            to_y[b, y] = pair_sum(b, y, slice(None))
            to_y_send(b, d, to_y.at[b, y], from_y.at[b, d - 1], y_peers[d])

    def relay_y(b):
        right_y, left_y = y_peers[1][1], y_peers[ny - 1][1]
        for lane, side, near_y, where, came in (
            (4, 1, right_y, halves[0], 0),
            (5, ny - 1, left_y, halves[1], 1),
        ):
            sum_y_copies[b, came].wait_recv()
            to_y[b, near_y, where, :] = pair_sum(b, near_y, where) + far_in[b, came]
            to_y_send(
                b, lane, to_y.at[b, near_y, where], from_y.at[b, lane - 4, where], y_peers[side]
            )

    def sum_over_z(b):
        for lane in range(1, ny) if b in DIRECT else range(2, 6):
            sum_y_copies[b, lane].wait_recv()
        value = part[b, my_c, my_y].astype(f32) + from_twin[b, my_y].astype(f32)
        for side in range(ny - 1 if b in DIRECT else 2):
            value = value + from_y[b, side].astype(f32)
        value = value.reshape(nz, r, half)
        of_y[b] = value
        to_z[b] = value.astype(bf)
        for d in range(1, nz):
            sum_z_copies[b, d] = start(
                to_z.at[b, z_peers[d][0]],
                from_z.at[b, d],
                rz_send.at[b, d],
                rz_recv.at[b, d],
                z_peers[d],
            )

    def finish(b):
        value = of_y[b, my_z]
        for d in range(1, nz):
            sum_z_copies[b, d].wait_recv()
            value = value + from_z[b, d].astype(f32)
        total[b] = value

    def first_y(b):
        (direct_y if b in DIRECT else sum_over_y)(b)

    def second_y(b):
        if b not in DIRECT:
            relay_y(b)

    def wait_left():
        d_near[0, 1].wait_recv()

    def wait_right():
        d_near[1, 0].wait_recv()

    def wait_far():
        for copy in d_far:
            copy.wait_recv()

    multiply(0)
    first_y(0)
    wait_left()
    multiply(1)
    first_y(1)
    second_y(0)
    wait_right()
    multiply(2)
    first_y(2)
    second_y(1)
    sum_over_z(0)
    wait_far()
    multiply(3)
    second_y(2)
    first_y(3)
    sum_over_z(1)
    second_y(3)
    finish(0)
    sum_over_z(2)
    finish(1)
    sum_over_z(3)
    finish(2)
    finish(3)

    own = mixed_out.shape[0]
    first_core = my_c == 0
    low, high = total[:, 0:own, :], total[:, own : 2 * own, :]
    other[...] = jnp.where(first_core, high, low)
    swap = start(other, last, t_send.at[len(blocks)], t_recv.at[len(blocks)], twin)
    mine = jnp.where(first_core, low, high)
    swap.wait_recv()
    theirs = last[...]
    for b, (x, offset) in enumerate(blocks):
        pair = [
            jnp.where(first_core, mine[b], theirs[b]),
            jnp.where(first_core, theirs[b], mine[b]),
        ]
        at_cols = pl.ds(pl.multiple_of(x * cols + offset, piece), piece)
        mixed_out[:, at_cols] = jnp.concatenate(pair, axis=1).astype(bf)
    for copy in sent:
        copy.wait_send()


def away(array):
    return pltpu.with_memory_space_constraint(array, pltpu.HBM)


def whole(sizes, gate_weight, up_weight, gain, down_weight, tokens, routes, logits):
    nz, ny, nc, nx = sizes
    nyc = ny * nc
    nk = nz * nyc
    per_x = nk // nx
    experts, rows, cols = gate_weight.shape
    width = cols // per_x
    hid, dcols = down_weight.shape[1:]
    bf, f32 = jnp.bfloat16, jnp.float32
    steps = nyc - 1
    count = tokens.shape[0]
    r = count // (nz * ny)
    nb = nx * SPLIT
    half = dcols // nc // SPLIT
    dma = pltpu.SemaphoreType.DMA
    vmem = pl.BlockSpec(memory_space=pltpu.VMEM)
    hbm = pl.BlockSpec(memory_space=pltpu.HBM)
    return pl.pallas_call(
        functools.partial(whole_kernel, sizes),
        out_shape=[
            pltpu.VMEM((experts, nz, nyc, rows, width), bf),
            pltpu.VMEM((experts, nz, nyc, rows, width), bf),
            pltpu.VMEM((experts, hid, dcols * nx), bf),
            pltpu.VMEM((count // nk, dcols * nx), bf),
        ],
        in_specs=[hbm] * 7,
        out_specs=[vmem] * 4,
        scratch_shapes=[
            pltpu.VMEM(gate_weight.shape, f32),
            pltpu.VMEM(up_weight.shape, f32),
            pltpu.VMEM(down_weight.shape, f32),
            pltpu.VMEM(tokens.shape, bf),
            pltpu.VMEM(gain.shape, f32),
            pltpu.VMEM(routes.shape, jnp.int32),
            pltpu.VMEM(logits.shape, f32),
            pltpu.VMEM((3, nx, per_x, rows // 2, width), bf),
            pltpu.VMEM((3, nk, rows // 2, width), bf),
            pltpu.VMEM((3, nz, nyc, rows // 2, width), bf),
            pltpu.VMEM((nx, per_x, rows // 4, width), bf),
            pltpu.VMEM((nk, rows // 4, width), bf),
            pltpu.VMEM((nz, nyc, rows // 4, width), bf),
            pltpu.VMEM((nx, nk, rows // 4, width), bf),
            pltpu.VMEM((nx, nz, nyc, rows // 4, width), bf),
            pltpu.VMEM(tokens.shape, bf),
            pltpu.VMEM((experts, count, hid), f32),
            pltpu.VMEM((experts, count, hid), bf),
            pltpu.VMEM((nb, nc, ny, nz * r, half), bf),
            pltpu.VMEM((nb, ny, nz * r, half), bf),
            pltpu.VMEM((nb, ny, nz * r, half), bf),
            pltpu.VMEM((nb, ny - 1, nz * r, half), bf),
            pltpu.VMEM((nb, 2, nz * r // 2, half), bf),
            pltpu.VMEM((nb, nz, r, half), f32),
            pltpu.VMEM((nb, nz, r, half), bf),
            pltpu.VMEM((nb, nz, r, half), bf),
            pltpu.VMEM((nb, r, half), f32),
            pltpu.VMEM((nb, r // nc, half), f32),
            pltpu.VMEM((nb, r // nc, half), f32),
            dma((7,)),
            dma((4, nx)),
            dma((4, nx)),
            dma((4, nz)),
            dma((4, nz)),
            dma((nx, nz)),
            dma((nx, nz)),
            dma((nx, steps)),
            dma((nx, steps)),
            dma((4, steps)),
            dma((4, steps)),
            dma((6, 2, 2)),
            dma((6, 2, 2)),
            dma((6, 2)),
            dma((6, 2)),
            dma((nb + 1,)),
            dma((nb + 1,)),
            dma((nb, 6)),
            dma((nb, 6)),
            dma((nb, nz)),
            dma((nb, nz)),
        ],
        compiler_params=pltpu.CompilerParams(
            collective_id=0, has_side_effects=True, vmem_limit_bytes=44 * MIB
        ),
        name="whole",
    )(*(away(a) for a in (gate_weight, up_weight, gain, down_weight, tokens, routes, logits)))


def write_kernel(*refs):
    count = len(refs) // 2
    copies = [
        pltpu.make_async_copy(refs[i], refs[count + i], refs[-1].at[i]) for i in range(count)
    ]
    for copy in copies:
        copy.start()
    for copy in copies:
        copy.wait()


def write_out(*arrays):
    return pl.pallas_call(
        write_kernel,
        out_shape=[jax.ShapeDtypeStruct(a.shape, a.dtype) for a in arrays],
        in_specs=[pl.BlockSpec(memory_space=pltpu.VMEM)] * len(arrays),
        out_specs=[pl.BlockSpec(memory_space=pltpu.HBM)] * len(arrays),
        scratch_shapes=[pltpu.SemaphoreType.DMA((len(arrays),))],
        compiler_params=pltpu.CompilerParams(vmem_limit_bytes=12 * MIB),
        name="write_out",
    )(*arrays)


def shards(sizes, tokens, norm_gain, gate_weight, up_weight, down_weight, routes, route_logit):
    gate, up, down, mixed = whole(
        sizes, gate_weight, up_weight, norm_gain[None, :], down_weight, tokens, routes.T, route_logit.T
    )
    full = (gate.shape[0], -1, gate.shape[-1])
    return tuple(write_out(gate.reshape(full), up.reshape(full), down, mixed))


def solution(mesh):
    sizes = (8, 4, 2, mesh.shape["tp"])
    finer = Mesh(mesh.devices.reshape(sizes), ("fs_0", "fs_1", "fs_2", "tp"))
    in_specs = (
        P("tp", None),
        P(FS),
        P(None, FS, "tp"),
        P(None, FS, "tp"),
        P(None, FS, "tp"),
        P("tp", None),
        P("tp", None),
    )
    out_specs = (P(None, None, FS), P(None, None, FS), P(None, FS, None), P(TP_FS, None))
    return jax.shard_map(
        functools.partial(shards, sizes),
        mesh=finer,
        in_specs=in_specs,
        out_specs=out_specs,
        check_vma=False,
    )
```

```python
import functools

import jax
import jax.numpy as jnp
from jax import lax
from jax.experimental import pallas as pl
from jax.experimental.pallas import tpu as pltpu
from jax.sharding import Mesh
from jax.sharding import PartitionSpec as P

FS = ("fs_0", "fs_1", "fs_2")
TP_FS = ("tp", "fs_0", "fs_1", "fs_2")
EPS = 0.5
MESH = pl.DeviceIdType.MESH
MIB = 1024 * 1024
SPLIT = 1
DIRECT = (3,)


def whole_kernel(
    sizes,
    gate_hbm,
    up_hbm,
    gain_hbm,
    down_hbm,
    token_hbm,
    route_hbm,
    logit_hbm,
    gate_out,
    up_out,
    down_out,
    mixed_out,
    gate_in,
    up_in,
    down_in,
    token_in,
    gain_ref,
    route_ref,
    logit_ref,
    staged,
    spread,
    by_z,
    staged_b,
    spread_b,
    by_z_b,
    wide,
    wide_by_z,
    normed,
    share,
    hidden,
    part,
    from_twin,
    to_y,
    from_y,
    far_in,
    of_y,
    to_z,
    from_z,
    total,
    other,
    last,
    in_sem,
    a_send,
    a_recv,
    z_send,
    z_recv,
    wz_send,
    wz_recv,
    wy_send,
    wy_recv,
    y_send,
    y_recv,
    c_send,
    c_recv,
    f_send,
    f_recv,
    t_send,
    t_recv,
    ry_send,
    ry_recv,
    rz_send,
    rz_recv,
):
    nz, ny, nc, nx = sizes
    nyc = ny * nc
    nk = nz * nyc
    per_x = nk // nx
    f32, bf = jnp.float32, jnp.bfloat16
    my_z, my_y = lax.axis_index("fs_0"), lax.axis_index("fs_1")
    my_c, my_x = lax.axis_index("fs_2"), lax.axis_index("tp")
    my_yc = my_y * nc + my_c
    outs = (gate_out, up_out)

    loads = [
        pltpu.make_async_copy(src, dst, in_sem.at[i])
        for i, (src, dst) in enumerate(
            (
                (gate_hbm, gate_in),
                (up_hbm, up_in),
                (down_hbm, down_in),
                (token_hbm, token_in),
                (gain_hbm, gain_ref),
                (route_hbm, route_ref),
                (logit_hbm, logit_ref),
            )
        )
    ]
    for i in (4, 0, 1, 2, 5, 6, 3):
        loads[i].start()

    def at(dz=0, dy=0, dc=0, dx=0):
        return (
            lax.rem(my_z + dz, nz),
            lax.rem(my_y + dy, ny),
            lax.rem(my_c + dc, nc),
            lax.rem(my_x + dx, nx),
        )

    yc_steps = [(dy, dc) for dy in range(ny) for dc in range(nc) if dy + dc > 0]
    peers = (
        [at(dx=d) for d in range(1, nx)]
        + [at(dz=d) for d in range(1, nz)]
        + [at(dy=dy, dc=dc) for dy, dc in yc_steps]
    )
    barrier = pltpu.get_barrier_semaphore()
    for peer in peers:
        pl.semaphore_signal(barrier, inc=1, device_id=peer, device_id_type=MESH)

    sent = []

    def start(src, dst, ssem, rsem, peer):
        copy = pltpu.make_async_remote_copy(
            src_ref=src, dst_ref=dst, send_sem=ssem, recv_sem=rsem, device_id=peer, device_id_type=MESH
        )
        copy.start()
        sent.append(copy)
        return copy

    rows = gate_in.shape[1]
    width = gate_in.shape[2] // per_x
    loads[4].wait()
    gain_row = gain_ref[...]
    same = lax.broadcasted_iota(jnp.int32, (rows, rows), 0) == lax.broadcasted_iota(
        jnp.int32, (rows, rows), 1
    )
    gain = jnp.sum(jnp.where(same, gain_row, 0.0), axis=1, keepdims=True)
    step_a, step_b = rows // 2, rows // 4
    chunks = [
        (0, 0, step_a),
        (0, step_a, step_a),
        (1, 0, step_a),
        (1, step_a, step_b),
        (1, step_a + step_b, step_b),
    ]
    stages = [(staged.at[i], spread.at[i], by_z.at[i]) for i in range(3)]
    stages.append((staged_b, spread_b, by_z_b))

    a_copies = {}
    for q, (m, lo, n) in enumerate(chunks):
        ref = (gate_in, up_in)[m]
        if lo == 0:
            loads[m].wait()
        for d in range(nx):
            expert = lax.rem(my_x + d, nx)
            for k in range(per_x):
                block = ref[expert, lo : lo + n, k * width : (k + 1) * width]
                block = (block * gain[lo : lo + n]).astype(bf)
                if q == len(chunks) - 1:
                    wide[expert, my_x * per_x + k] = block
                elif d == 0:
                    stages[q][1][my_x * per_x + k] = block
                else:
                    stages[q][0][d, k] = block
        if q == 0:
            pl.semaphore_wait(barrier, len(peers))
        if q == len(chunks) - 1:
            continue
        for d in range(1, nx):
            a_copies[q, d] = start(
                stages[q][0].at[d],
                stages[q][1].at[pl.ds(my_x * per_x, per_x)],
                a_send.at[q, d],
                a_recv.at[q, d],
                at(dx=d),
            )

    cols = down_in.shape[2]
    half_e = nx // 2
    loads[2].wait()
    own_cols = pl.ds(pl.multiple_of(my_x * cols, cols), cols)
    for e in range(nx):
        down_out[e, :, own_cols] = down_in[e].astype(bf)

    left, right = lax.rem(my_x + nx - 1, nx), lax.rem(my_x + 1, nx)

    def near(tag, block, side, h):
        ref = block(my_x, h)
        return start(
            ref, ref, c_send.at[tag, side, h], c_recv.at[tag, side, h], at(dx=1 if side == 0 else nx - 1)
        )

    def pass_on(tag, block, side):
        ref = block(left if side == 0 else right, side)
        return start(
            ref, ref, f_send.at[tag, side], f_recv.at[tag, side], at(dx=1 if side == 0 else nx - 1)
        )

    def down_block(x, h):
        return down_out.at[
            pl.ds(h * half_e, half_e), :, pl.ds(pl.multiple_of(x * cols, cols), cols)
        ]

    def near_all(tag, block):
        copies = {(s, s): near(tag, block, s, s) for s in (0, 1)}
        copies.update({(s, 1 - s): near(tag, block, s, 1 - s) for s in (0, 1)})
        return copies

    def wide_block(x, h):
        return wide.at[
            pl.ds(h * half_e, half_e), pl.ds(pl.multiple_of(x * per_x, per_x), per_x)
        ]

    w_tag, d_tag = len(chunks) - 1, len(chunks)
    w_near = near_all(w_tag, wide_block)

    loads[3].wait()
    step = 48

    def norm_rows(i, carry):
        at_rows = pl.ds(pl.multiple_of(i * step, step), step)
        floats = token_in[at_rows, :].astype(f32)
        scale = lax.rsqrt(jnp.mean(floats * floats, axis=1, keepdims=True) + EPS)
        normed[at_rows, :] = (floats * scale).astype(bf)
        return carry

    lax.fori_loop(0, token_in.shape[0] // step, norm_rows, 0)
    loads[5].wait()
    loads[6].wait()
    first = 1.0 / (1.0 + jnp.exp(logit_ref[1:2, :] - logit_ref[0:1, :]))
    lines = [
        jnp.where(route_ref[0:1, :] == e, first, 0.0)
        + jnp.where(route_ref[1:2, :] == e, 1.0 - first, 0.0)
        for e in range(nx)
    ]
    lines.append(jnp.zeros((128 - nx, first.shape[1]), f32))
    columns = jnp.concatenate(lines, axis=0).T
    for e in range(nx):
        share[e] = jnp.broadcast_to(columns[:, e : e + 1], share.shape[1:])

    z_copies, y_copies, c_near, c_far = {}, {}, {}, {}
    half_z = nz // 2

    def over_z(q):
        _, by_x, by_z_q = stages[q]
        for d in range(1, nx):
            a_copies[q, d].wait_recv()
        for dz in range(1, nz):
            peer = at(dz=dz)
            z_copies[q, dz] = start(
                by_x.at[pl.ds(peer[0] * nyc, nyc)],
                by_z_q.at[my_z],
                z_send.at[q, dz],
                z_recv.at[q, dz],
                peer,
            )
        by_z_q[my_z] = by_x[pl.ds(my_z * nyc, nyc)]

    def over_yc(q):
        m, lo, n = chunks[q]
        out, by_z_q = outs[m], stages[q][2]
        for dz in range(1, nz):
            z_copies[q, dz].wait_recv()
        for i, (dy, dc) in enumerate(yc_steps):
            peer = at(dy=dy, dc=dc)
            y_copies[q, i] = start(
                by_z_q.at[:, peer[1] * nc + peer[2]],
                out.at[my_x, :, my_yc, pl.ds(lo, n)],
                y_send.at[q, i],
                y_recv.at[q, i],
                peer,
            )
        out[my_x, :, my_yc, lo : lo + n, :] = by_z_q[:, my_yc]

    def out_block(q):
        m, lo, n = chunks[q]
        return lambda x, half: outs[m].at[x, pl.ds(half * half_z, half_z), :, pl.ds(lo, n)]

    def over_x(q):
        tag = q
        for i in range(len(yc_steps)):
            y_copies[q, i].wait_recv()
        for s in (0, 1):
            c_near[q, s, s] = near(tag, out_block(q), s, s)
        for s in (0, 1):
            c_near[q, s, 1 - s] = near(tag, out_block(q), s, 1 - s)

    def onward(q):
        for s in (0, 1):
            c_near[q, s, s].wait_recv()
            c_far[q, s] = pass_on(q, out_block(q), s)

    experts = nx
    hid = width
    tiles = 2
    tile_rows = normed.shape[0] // tiles
    z_per = nz // tiles
    r = normed.shape[0] // (nz * ny)

    def run_expert(e):
        def tile(t, carry):
            at_rows = pl.ds(pl.multiple_of(t * tile_rows, tile_rows), tile_rows)
            shape = (nk * rows, width)
            both = jnp.concatenate([gate_out[e].reshape(shape), up_out[e].reshape(shape)], axis=1)
            val = jnp.dot(normed[at_rows, :], both, preferred_element_type=f32)
            gate_val, up_val = val[:, :hid], val[:, hid:]
            weight = share[e, at_rows, :]
            value = gate_val / (1.0 + jnp.exp(-gate_val)) * up_val
            hidden[e, at_rows, :] = jnp.where(weight > 0.0, value * weight, 0.0).astype(bf)
            return carry

        lax.fori_loop(0, tiles, tile, 0)

    order = [my_x, left, right, lax.rem(my_x + nx // 2, nx)]
    w_out, w_lo, sub = outs[chunks[-1][0]], chunks[-1][1], chunks[-1][2]
    wz_copies, wy_copies = {}, {}

    def wide_over_z():
        for s in (0, 1):
            w_near[s, 1 - s].wait_recv()
        for copy in w_onward:
            copy.wait_recv()
        for i, e in enumerate(order):
            for dz in range(1, nz):
                peer = at(dz=dz)
                wz_copies[i, dz] = start(
                    wide.at[e, pl.ds(peer[0] * nyc, nyc)],
                    wide_by_z.at[e, my_z],
                    wz_send.at[i, dz],
                    wz_recv.at[i, dz],
                    peer,
                )
            wide_by_z[e, my_z] = wide[e, pl.ds(my_z * nyc, nyc)]

    def wide_over_yc(i):
        e = order[i]
        for dz in range(1, nz):
            wz_copies[i, dz].wait_recv()
        for j, (dy, dc) in enumerate(yc_steps):
            peer = at(dy=dy, dc=dc)
            wy_copies[i, j] = start(
                wide_by_z.at[e, :, peer[1] * nc + peer[2]],
                w_out.at[e, :, my_yc, pl.ds(w_lo, sub)],
                wy_send.at[i, j],
                wy_recv.at[i, j],
                peer,
            )
        w_out[e, :, my_yc, w_lo : w_lo + sub, :] = wide_by_z[e, :, my_yc]

    def wide_done(i):
        for j in range(len(yc_steps)):
            wy_copies[i, j].wait_recv()

    over_z(0)
    over_z(1)
    over_z(2)
    over_yc(0)
    over_z(3)
    w_onward = []
    for s in (0, 1):
        w_near[s, s].wait_recv()
        w_onward.append(pass_on(w_tag, wide_block, s))
    d_near = {(s, s): near(d_tag, down_block, s, s) for s in (0, 1)}
    over_x(0)
    over_yc(1)
    wide_over_z()
    over_yc(2)
    over_x(1)
    onward(0)
    over_yc(3)
    over_x(2)
    wide_over_yc(0)
    over_x(3)
    onward(1)
    wide_over_yc(1)
    wide_done(0)
    run_expert(order[0])
    wide_over_yc(2)
    wide_over_yc(3)
    onward(2)
    onward(3)
    for s in (0, 1):
        d_near[s, 1 - s] = near(d_tag, down_block, s, 1 - s)
    d_far = []
    for s in (0, 1):
        d_near[s, s].wait_recv()
        d_far.append(pass_on(d_tag, down_block, s))
    for i, s in ((1, 0), (2, 1)):
        wide_done(i)
        for q in range(4):
            c_near[q, s, 1 - s].wait_recv()
        run_expert(order[i])
    wide_done(3)
    for q in range(4):
        for s in (0, 1):
            c_far[q, s].wait_recv()
    run_expert(order[3])

    early = len(sent) - 2
    piece = cols // SPLIT
    half = piece // nc
    twin = at(dc=1)
    y_peers = [at(dy=d) for d in range(ny)]
    z_peers = [at(dz=d) for d in range(nz)]
    owners = [my_x, left, right, lax.rem(my_x + nx // 2, nx)]
    blocks = [(x, i * piece) for x in owners for i in range(SPLIT)]
    twin_copies, sum_y_copies, sum_z_copies = {}, {}, {}

    def multiply(b):
        x, offset = blocks[b]
        at_cols = pl.ds(pl.multiple_of(x * cols + offset, piece), piece)

        def tile(t, carry):
            at_rows = pl.ds(pl.multiple_of(t * tile_rows, tile_rows), tile_rows)
            units = jnp.concatenate([hidden[e, at_rows, :] for e in range(experts)], axis=1)
            down = down_out[:, :, at_cols].reshape(experts * hid, piece)
            val = jnp.dot(units, down, preferred_element_type=f32)
            val = val.reshape(z_per, ny, r, piece)
            at_part = pl.ds(pl.multiple_of(t * z_per * r, z_per * r), z_per * r)
            for y in range(ny):
                lines = jnp.concatenate([val[z, y] for z in range(z_per)], axis=0).astype(bf)
                for c in range(nc):
                    part[b, c, y, at_part, :] = lines[:, c * half : (c + 1) * half]
            return carry

        lax.fori_loop(0, tiles, tile, 0)
        twin_copies[b] = start(
            part.at[b, twin[2]], from_twin.at[b], t_send.at[b], t_recv.at[b], twin
        )

    far_y = ny // 2
    count_y = nz * r
    halves = (pl.ds(0, count_y // 2), pl.ds(count_y // 2, count_y // 2))

    def to_y_send(b, lane, part_of, landing, target):
        sum_y_copies[b, lane] = start(
            part_of, landing, ry_send.at[b, lane], ry_recv.at[b, lane], target
        )

    def pair_sum(b, y, where):
        return part[b, my_c, y, where, :] + from_twin[b, y, where, :]

    def sum_over_y(b):
        twin_copies[b].wait_recv()
        right_y, far, left_y = (y_peers[d][1] for d in (1, far_y, ny - 1))
        for lane, side in ((0, 1), (1, ny - 1)):
            to_y[b, far, halves[lane], :] = pair_sum(b, far, halves[lane])
            to_y_send(
                b, lane, to_y.at[b, far, halves[lane]], far_in.at[b, lane], y_peers[side]
            )
        for lane, side, near_y, where in (
            (2, 1, right_y, halves[1]),
            (3, ny - 1, left_y, halves[0]),
        ):
            to_y[b, near_y, where, :] = pair_sum(b, near_y, where)
            to_y_send(
                b, lane, to_y.at[b, near_y, where], from_y.at[b, lane - 2, where], y_peers[side]
            )

    def direct_y(b):
        twin_copies[b].wait_recv()
        for d in (far_y, 1, ny - 1):
            y = y_peers[d][1]
            to_y[b, y] = pair_sum(b, y, slice(None))
            to_y_send(b, d, to_y.at[b, y], from_y.at[b, d - 1], y_peers[d])

    def relay_y(b):
        right_y, left_y = y_peers[1][1], y_peers[ny - 1][1]
        for lane, side, near_y, where, came in (
            (4, 1, right_y, halves[0], 0),
            (5, ny - 1, left_y, halves[1], 1),
        ):
            sum_y_copies[b, came].wait_recv()
            to_y[b, near_y, where, :] = pair_sum(b, near_y, where) + far_in[b, came]
            to_y_send(
                b, lane, to_y.at[b, near_y, where], from_y.at[b, lane - 4, where], y_peers[side]
            )

    def sum_over_z(b):
        for lane in range(1, ny) if b in DIRECT else range(2, 6):
            sum_y_copies[b, lane].wait_recv()
        value = part[b, my_c, my_y].astype(f32) + from_twin[b, my_y].astype(f32)
        for side in range(ny - 1 if b in DIRECT else 2):
            value = value + from_y[b, side].astype(f32)
        value = value.reshape(nz, r, half)
        of_y[b] = value
        to_z[b] = value.astype(bf)
        for d in range(1, nz):
            sum_z_copies[b, d] = start(
                to_z.at[b, z_peers[d][0]],
                from_z.at[b, d],
                rz_send.at[b, d],
                rz_recv.at[b, d],
                z_peers[d],
            )

    def finish(b):
        value = of_y[b, my_z]
        for d in range(1, nz):
            sum_z_copies[b, d].wait_recv()
            value = value + from_z[b, d].astype(f32)
        total[b] = value

    def first_y(b):
        (direct_y if b in DIRECT else sum_over_y)(b)

    def second_y(b):
        if b not in DIRECT:
            relay_y(b)

    def wait_left():
        d_near[0, 1].wait_recv()

    def wait_right():
        d_near[1, 0].wait_recv()

    def wait_far():
        for copy in d_far:
            copy.wait_recv()

    multiply(0)
    first_y(0)
    wait_left()
    multiply(1)
    first_y(1)
    second_y(0)
    wait_right()
    multiply(2)
    first_y(2)
    second_y(1)
    sum_over_z(0)
    for copy in sent[:early]:
        copy.wait_send()
    del sent[:early]
    wait_far()
    multiply(3)
    second_y(2)
    first_y(3)
    sum_over_z(1)
    second_y(3)
    finish(0)
    sum_over_z(2)
    finish(1)
    sum_over_z(3)
    finish(2)
    finish(3)

    own = mixed_out.shape[0]
    first_core = my_c == 0
    low, high = total[:, 0:own, :], total[:, own : 2 * own, :]
    other[...] = jnp.where(first_core, high, low)
    swap = start(other, last, t_send.at[len(blocks)], t_recv.at[len(blocks)], twin)
    mine = jnp.where(first_core, low, high)
    swap.wait_recv()
    theirs = last[...]
    for b, (x, offset) in enumerate(blocks):
        pair = [
            jnp.where(first_core, mine[b], theirs[b]),
            jnp.where(first_core, theirs[b], mine[b]),
        ]
        at_cols = pl.ds(pl.multiple_of(x * cols + offset, piece), piece)
        mixed_out[:, at_cols] = jnp.concatenate(pair, axis=1).astype(bf)
    for copy in sent:
        copy.wait_send()


def away(array):
    return pltpu.with_memory_space_constraint(array, pltpu.HBM)


def whole(sizes, gate_weight, up_weight, gain, down_weight, tokens, routes, logits):
    nz, ny, nc, nx = sizes
    nyc = ny * nc
    nk = nz * nyc
    per_x = nk // nx
    experts, rows, cols = gate_weight.shape
    width = cols // per_x
    hid, dcols = down_weight.shape[1:]
    bf, f32 = jnp.bfloat16, jnp.float32
    steps = nyc - 1
    count = tokens.shape[0]
    r = count // (nz * ny)
    nb = nx * SPLIT
    half = dcols // nc // SPLIT
    dma = pltpu.SemaphoreType.DMA
    vmem = pl.BlockSpec(memory_space=pltpu.VMEM)
    hbm = pl.BlockSpec(memory_space=pltpu.HBM)
    return pl.pallas_call(
        functools.partial(whole_kernel, sizes),
        out_shape=[
            pltpu.VMEM((experts, nz, nyc, rows, width), bf),
            pltpu.VMEM((experts, nz, nyc, rows, width), bf),
            pltpu.VMEM((experts, hid, dcols * nx), bf),
            pltpu.VMEM((count // nk, dcols * nx), bf),
        ],
        in_specs=[hbm] * 7,
        out_specs=[vmem] * 4,
        scratch_shapes=[
            pltpu.VMEM(gate_weight.shape, f32),
            pltpu.VMEM(up_weight.shape, f32),
            pltpu.VMEM(down_weight.shape, f32),
            pltpu.VMEM(tokens.shape, bf),
            pltpu.VMEM(gain.shape, f32),
            pltpu.VMEM(routes.shape, jnp.int32),
            pltpu.VMEM(logits.shape, f32),
            pltpu.VMEM((3, nx, per_x, rows // 2, width), bf),
            pltpu.VMEM((3, nk, rows // 2, width), bf),
            pltpu.VMEM((3, nz, nyc, rows // 2, width), bf),
            pltpu.VMEM((nx, per_x, rows // 4, width), bf),
            pltpu.VMEM((nk, rows // 4, width), bf),
            pltpu.VMEM((nz, nyc, rows // 4, width), bf),
            pltpu.VMEM((nx, nk, rows // 4, width), bf),
            pltpu.VMEM((nx, nz, nyc, rows // 4, width), bf),
            pltpu.VMEM(tokens.shape, bf),
            pltpu.VMEM((experts, count, hid), f32),
            pltpu.VMEM((experts, count, hid), bf),
            pltpu.VMEM((nb, nc, ny, nz * r, half), bf),
            pltpu.VMEM((nb, ny, nz * r, half), bf),
            pltpu.VMEM((nb, ny, nz * r, half), bf),
            pltpu.VMEM((nb, ny - 1, nz * r, half), bf),
            pltpu.VMEM((nb, 2, nz * r // 2, half), bf),
            pltpu.VMEM((nb, nz, r, half), f32),
            pltpu.VMEM((nb, nz, r, half), bf),
            pltpu.VMEM((nb, nz, r, half), bf),
            pltpu.VMEM((nb, r, half), f32),
            pltpu.VMEM((nb, r // nc, half), f32),
            pltpu.VMEM((nb, r // nc, half), f32),
            dma((7,)),
            dma((4, nx)),
            dma((4, nx)),
            dma((4, nz)),
            dma((4, nz)),
            dma((nx, nz)),
            dma((nx, nz)),
            dma((nx, steps)),
            dma((nx, steps)),
            dma((4, steps)),
            dma((4, steps)),
            dma((6, 2, 2)),
            dma((6, 2, 2)),
            dma((6, 2)),
            dma((6, 2)),
            dma((nb + 1,)),
            dma((nb + 1,)),
            dma((nb, 6)),
            dma((nb, 6)),
            dma((nb, nz)),
            dma((nb, nz)),
        ],
        compiler_params=pltpu.CompilerParams(
            collective_id=0, has_side_effects=True, vmem_limit_bytes=44 * MIB
        ),
        name="whole",
    )(*(away(a) for a in (gate_weight, up_weight, gain, down_weight, tokens, routes, logits)))


def write_kernel(*refs):
    count = len(refs) // 2
    copies = [
        pltpu.make_async_copy(refs[i], refs[count + i], refs[-1].at[i]) for i in range(count)
    ]
    for copy in copies:
        copy.start()
    for copy in copies:
        copy.wait()


def write_out(*arrays):
    return pl.pallas_call(
        write_kernel,
        out_shape=[jax.ShapeDtypeStruct(a.shape, a.dtype) for a in arrays],
        in_specs=[pl.BlockSpec(memory_space=pltpu.VMEM)] * len(arrays),
        out_specs=[pl.BlockSpec(memory_space=pltpu.HBM)] * len(arrays),
        scratch_shapes=[pltpu.SemaphoreType.DMA((len(arrays),))],
        compiler_params=pltpu.CompilerParams(vmem_limit_bytes=12 * MIB),
        name="write_out",
    )(*arrays)


def shards(sizes, tokens, norm_gain, gate_weight, up_weight, down_weight, routes, route_logit):
    gate, up, down, mixed = whole(
        sizes, gate_weight, up_weight, norm_gain[None, :], down_weight, tokens, routes.T, route_logit.T
    )
    full = (gate.shape[0], -1, gate.shape[-1])
    return tuple(write_out(gate.reshape(full), up.reshape(full), down, mixed))


def solution(mesh):
    sizes = (8, 4, 2, mesh.shape["tp"])
    finer = Mesh(mesh.devices.reshape(sizes), ("fs_0", "fs_1", "fs_2", "tp"))
    in_specs = (
        P("tp", None),
        P(FS),
        P(None, FS, "tp"),
        P(None, FS, "tp"),
        P(None, FS, "tp"),
        P("tp", None),
        P("tp", None),
    )
    out_specs = (P(None, None, FS), P(None, None, FS), P(None, FS, None), P(TP_FS, None))
    return jax.shard_map(
        functools.partial(shards, sizes),
        mesh=finer,
        in_specs=in_specs,
        out_specs=out_specs,
        check_vma=False,
    )
```
